32 devices in a mesh: ep: 32 (over z, y, x, core).
Axes of the slice: x: 2, y: 2, z: 4, core: 2. Of those that a mesh axis runs over, the one named last changes fastest.
Arguments:
- tokens: bfloat16 [256, 2048], P('ep'), may hold values from -6 to 6
- premix_gain: float32 [2048], replicated, may hold values from 0.1 to 1.9
- postmix_gain: float32 [2048], replicated, may hold values from 0.1 to 1.9
- prefeed_gain: float32 [2048], replicated, may hold values from 0.1 to 1.9
- postfeed_gain: float32 [2048], replicated, may hold values from 0.1 to 1.9
- query_weight: bfloat16 [2048, 1024], P('ep'), may hold values from -0.125 to 0.125
- key_weight: bfloat16 [2048, 1024], P('ep'), may hold values from -0.125 to 0.125
- value_weight: bfloat16 [2048, 1024], P('ep'), may hold values from -0.125 to 0.125
- outgate_weight: bfloat16 [2048, 1024], P('ep'), may hold values from -0.125 to 0.125
- ingate_weight: bfloat16 [2048, 8], replicated, may hold values from -0.125 to 0.125
- forget_weight: bfloat16 [2048, 8], replicated, may hold values from -0.125 to 0.125
- ingate_bias: float32 [8], replicated, may hold values from -1 to 1
- forget_bias: float32 [8], replicated, may hold values from -1 to 5
- memory_state: float32 [256, 8, 128, 128], P('ep'), may hold values from -1.25 to 1.25
- normalizer: float32 [256, 8, 128], P('ep'), may hold values from -1.75 to 1.75
- stabilizer: float32 [256, 8], P('ep'), may hold values from -2 to 2
- output_weight: bfloat16 [1024, 2048], P(None, 'ep'), may hold values from -0.1875 to 0.1875
- expert_ids: int32 [256, 6], P('ep'), may hold values from 0 to 31, all different within a row; in each aligned block of 8 rows (0 to 7, 8 to 15, ...) at most 4 rows name the same one
- route_weights: float32 [256, 6], P('ep'), may hold values from 0.2 to 0.8
- expert_gate: bfloat16 [32, 2048, 512], P('ep'), may hold values from -0.125 to 0.125
- expert_up: bfloat16 [32, 2048, 512], P('ep'), may hold values from -0.125 to 0.125
- expert_down: bfloat16 [32, 512, 2048], P('ep'), may hold values from -0.25 to 0.25
- shared_gate: bfloat16 [2048, 512], replicated, may hold values from -0.125 to 0.125
- shared_up: bfloat16 [2048, 512], replicated, may hold values from -0.125 to 0.125
- shared_down: bfloat16 [512, 2048], replicated, may hold values from -0.25 to 0.25
Outputs:
- next_tokens: bfloat16 [256, 2048], P('ep')
- next_memory: float32 [256, 8, 128, 128], P('ep')
- next_normalizer: float32 [256, 8, 128], P('ep')
- next_stabilizer: float32 [256, 8], P('ep')
The draws below stay inside these ranges and needn't reach their ends.
Inputs may be any that keep to these rules, and one draw needn't show every extreme that they name: `expert_ids`: each row names 6 different experts. Among the rows of one device no expert is named more than 4 times, and in every draw some expert is named exactly 4 times by the rows of some device.
All inputs are finite; a program needn't handle non-finite values.
Results may differ from the reference program's by a relative error of at most 0.0097.
Values may be sent and summed in bfloat16 or wider, within the bound.
No kernel may reach another device: no remote copies, remote signals or barrier semaphores. Data moves between devices by JAX's collectives and lax.ppermute only.
A program may use at most 128 MiB of HBM per device.

```python
import math
import jax
import jax.numpy as jnp
import numpy as np
from jax import lax

D = 2048
HEADS = 8
HEAD_DIM = 128
D_MEM = 1024
FF = 512
TOP_K = 6
EXPERTS = 32
SEQ_DEV = 8
SEQS = 256
CAP = 4
N_EP = 32


def block_scale(stream_key, extent, split, smallest, top_value):
    factor_of, own = 1.0, jax.random.fold_in(stream_key, 6)
    for axis_at, shards_of in split:
        heights = jnp.exp(jax.random.uniform(jax.random.fold_in(own, axis_at), (shards_of,), jnp.float32, smallest / len(split), top_value / len(split)))
        factor_of = factor_of * jnp.repeat(heights, extent[axis_at] // shards_of).reshape([-1 if axis == axis_at else 1 for axis in range(len(extent))])
    return factor_of


def deal_out(rng, own, number, rows, number_of, top, limit, slope):
    sequence = jax.random.permutation(rng, number_of)
    crowded, usual = portions_of(number_of, rows * top, limit, slope, True), portions_of(number_of, rows * top, limit, slope, False)
    places = jnp.arange(number_of)

    def named(lengths, rotation):
        used = int((lengths > 0).sum())
        fixed = max(1, used // 4)
        shifted = fixed + (places - fixed + rotation * (used - fixed)) % max(1, number_of - fixed)
        return jnp.zeros((number_of,), jnp.int32).at[sequence[jnp.where(places < fixed, places, shifted)]].set(jnp.asarray(lengths, jnp.int32))

    lengths = jnp.where(number % 4 == 0, named(crowded, number // 4), named(usual, number - number // 4 - 1))
    mixed = jax.random.permutation(jax.random.fold_in(own, 3), number_of)
    donor, taker = mixed[0:number_of // 2 * 2:2], mixed[1:number_of // 2 * 2:2]
    margin = jnp.minimum(lengths[donor] - 1, limit - lengths[taker]) // 2
    margin = jnp.where((donor == sequence[0]) | (taker == sequence[0]) | (lengths[taker] == 0), 0, jnp.maximum(margin, 0))
    shifted = jax.random.randint(jax.random.fold_in(own, 4), (number_of // 2,), 0, 1 << 20) % (margin + 1)
    lengths = lengths.at[donor].add(-shifted).at[taker].add(shifted)
    labels = jnp.searchsorted(jnp.cumsum(lengths), jnp.arange(rows * top), side="right").astype(jnp.int32)
    listing = labels.reshape(top, rows).T
    listing = listing[jax.random.permutation(jax.random.fold_in(own, 1), rows)]
    rotation = jax.random.randint(jax.random.fold_in(own, 2), (rows, 1), 0, top)
    return jnp.take_along_axis(listing, (jnp.arange(top)[None, :] + rotation) % top, axis=1)


def portions_of(number_of, total, limit, skew, full):
    weights = [(1 << 20) // math.isqrt(rank ** skew) + 1 for rank in range(1, number_of + 1)]
    largest = limit if full else min(limit, max(-(-total // number_of), total * weights[0] // sum(weights)))
    least = 1 if total - largest >= number_of - 1 else 0
    given, rest = [largest] + [least] * (number_of - 1), total - largest - least * (number_of - 1)
    while rest > 0:
        free = [i for i in range(1, number_of) if given[i] < largest] or [i for i in range(1, number_of) if given[i] < limit]
        pool, left = sum([weights[i] for i in free]), rest
        for i in free:
            addition = min(limit - given[i], max(1, left * weights[i] // pool), rest)
            given[i] = given[i] + addition
            rest = rest - addition
    return np.array(given)


def noise(own_key, extent, scale, bound, shards=(), kind=jnp.bfloat16):
    result = scale * jax.random.normal(own_key, extent, jnp.float32)
    if shards:
        result = result * block_scale(own_key, extent, shards, -0.22, 0.18)
    return jnp.clip(result, -bound, bound).astype(kind)


def setup_inputs(seed: int = 0) -> dict:
    streams_of = jax.random.split(jax.random.key(seed), 26)
    tokens = noise(streams_of[0], (SEQS, D), 1.0, 6.0, ((0, 32),))
    premix_gain = jnp.clip(1.0 + 0.18 * jax.random.normal(streams_of[1], (D,), jnp.float32), 0.1, 1.9)
    postmix_gain = jnp.clip(1.0 + 0.18 * jax.random.normal(streams_of[2], (D,), jnp.float32), 0.1, 1.9)
    prefeed_gain = jnp.clip(1.0 + 0.18 * jax.random.normal(streams_of[3], (D,), jnp.float32), 0.1, 1.9)
    postfeed_gain = jnp.clip(1.0 + 0.18 * jax.random.normal(streams_of[4], (D,), jnp.float32), 0.1, 1.9)
    query_weight = noise(streams_of[5], (D, D_MEM), D ** -0.5, 0.125, ((0, 32),))
    key_weight = noise(streams_of[6], (D, D_MEM), D ** -0.5, 0.125, ((0, 32),))
    value_weight = noise(streams_of[7], (D, D_MEM), D ** -0.5, 0.125, ((0, 32),))
    outgate_weight = noise(streams_of[8], (D, D_MEM), D ** -0.5, 0.125, ((0, 32),))
    ingate_weight = noise(streams_of[9], (D, HEADS), D ** -0.5, 0.125)
    forget_weight = noise(streams_of[10], (D, HEADS), D ** -0.5, 0.125)
    ingate_bias = jnp.clip(jax.random.uniform(streams_of[11], (HEADS,), jnp.float32, -1.0, 1.0), -1.0, 1.0)
    forget_bias = jnp.clip(jax.random.uniform(streams_of[12], (HEADS,), jnp.float32, -1.0, 5.0), -1.0, 5.0)
    memory_state = noise(streams_of[13], (SEQS, HEADS, HEAD_DIM, HEAD_DIM), 0.2, 1.25, ((0, 32),), jnp.float32)
    normalizer = noise(streams_of[14], (SEQS, HEADS, HEAD_DIM), 0.3, 1.75, ((0, 32),), jnp.float32)
    stabilizer = jnp.clip(jax.random.uniform(streams_of[15], (SEQS, HEADS), jnp.float32, -2.0, 2.0) * block_scale(streams_of[15], (SEQS, HEADS), ((0, 32),), -0.4, 0.0), -2.0, 2.0)
    output_weight = noise(streams_of[16], (D_MEM, D), D_MEM ** -0.5, 0.1875, ((1, 32),))
    expert_ids_keys = jax.random.split(jax.random.fold_in(streams_of[17], 1), SEQS // SEQ_DEV)
    expert_ids_turns = jax.random.permutation(jax.random.fold_in(streams_of[17], 3), SEQS // SEQ_DEV)
    expert_ids = jax.vmap(lambda own, number: deal_out(jax.random.fold_in(streams_of[17], 2), own, number, SEQ_DEV, EXPERTS, TOP_K, CAP, 2))(expert_ids_keys, expert_ids_turns).reshape((SEQS, TOP_K))
    route_weights = jnp.clip(0.2 + 0.6 * jax.random.uniform(streams_of[18], (SEQS, TOP_K), jnp.float32) ** block_scale(streams_of[18], (SEQS, TOP_K), ((0, 32),), -0.2, 0.2), 0.2, 0.8)
    expert_gate = noise(streams_of[19], (EXPERTS, D, FF), D ** -0.5, 0.125, ((0, 32),))
    expert_up = noise(streams_of[20], (EXPERTS, D, FF), D ** -0.5, 0.125, ((0, 32),))
    expert_down = noise(streams_of[21], (EXPERTS, FF, D), FF ** -0.5, 0.25, ((0, 32),))
    shared_gate = noise(streams_of[22], (D, FF), D ** -0.5, 0.125)
    shared_up = noise(streams_of[23], (D, FF), D ** -0.5, 0.125)
    shared_down = noise(streams_of[24], (FF, D), FF ** -0.5, 0.25)
    return dict(tokens=tokens, premix_gain=premix_gain, postmix_gain=postmix_gain, prefeed_gain=prefeed_gain, postfeed_gain=postfeed_gain, query_weight=query_weight, key_weight=key_weight, value_weight=value_weight, outgate_weight=outgate_weight, ingate_weight=ingate_weight, forget_weight=forget_weight, ingate_bias=ingate_bias, forget_bias=forget_bias, memory_state=memory_state, normalizer=normalizer, stabilizer=stabilizer, output_weight=output_weight, expert_ids=expert_ids, route_weights=route_weights, expert_gate=expert_gate, expert_up=expert_up, expert_down=expert_down, shared_gate=shared_gate, shared_up=shared_up, shared_down=shared_down)


epsilon = 1e-06

def rms_scale(values, gain_row):
    return values * lax.rsqrt(lax.optimization_barrier(jnp.mean(values * values, axis=-1, keepdims=True)) + epsilon) * gain_row

def rounded(values):
    return lax.optimization_barrier(values.astype(jnp.bfloat16))

def memory_step(queries, key_rows, value_rows, out_gate, input_pre, forget_pre, memory_state, normalizer, stabilizer):
    sequences = queries.shape[0]
    head_count = memory_state.shape[1]
    head_width = memory_state.shape[2]
    query_heads = queries.astype(jnp.float32).reshape(sequences, head_count, head_width)
    key_heads = key_rows.astype(jnp.float32).reshape(sequences, head_count, head_width) * head_width ** (-0.5)
    value_heads = value_rows.astype(jnp.float32).reshape(sequences, head_count, head_width)
    carried = jax.nn.log_sigmoid(forget_pre) + stabilizer
    next_stabilizer = jnp.maximum(carried, input_pre)
    keep_old = jnp.exp(carried - next_stabilizer)
    write_new = jnp.exp(input_pre - next_stabilizer)
    local_score = write_new * lax.optimization_barrier(jnp.sum(query_heads * key_heads, axis=-1))
    read_memory = jnp.einsum('shvk,shk->shv', memory_state, query_heads, precision=lax.Precision.HIGHEST)
    numerator = keep_old[..., None] * read_memory + local_score[..., None] * value_heads
    denominator = keep_old * lax.optimization_barrier(jnp.sum(normalizer * query_heads, axis=-1)) + local_score
    memory_read = numerator / jnp.maximum(jnp.abs(denominator), 1.0)[..., None]
    gated_out = (jax.nn.sigmoid(out_gate.astype(jnp.float32)) * memory_read.reshape(sequences, head_count * head_width)).astype(jnp.bfloat16)
    next_memory = keep_old[..., None, None] * memory_state + write_new[..., None, None] * value_heads[..., :, None] * key_heads[..., None, :]
    next_normalizer = keep_old[..., None] * normalizer + write_new[..., None] * key_heads
    return (gated_out, next_memory, next_normalizer, next_stabilizer)

def expert_rows(row_block, gate_weight, up_weight, down_weight):
    gate_values = jnp.dot(row_block, gate_weight, preferred_element_type=jnp.float32)
    up_values = jnp.dot(row_block, up_weight, preferred_element_type=jnp.float32)
    inner_rows = (jax.nn.silu(gate_values) * up_values).astype(jnp.bfloat16)
    return jnp.dot(inner_rows, down_weight, preferred_element_type=jnp.float32)

def reference(tokens, premix_gain, postmix_gain, prefeed_gain, postfeed_gain, query_weight, key_weight, value_weight, outgate_weight, ingate_weight, forget_weight, ingate_bias, forget_bias, memory_state, normalizer, stabilizer, output_weight, expert_ids, route_weights, expert_gate, expert_up, expert_down, shared_gate, shared_up, shared_down):
    residual = tokens.astype(jnp.float32)
    normed = rms_scale(residual, premix_gain).astype(jnp.bfloat16)
    queries = rounded(jnp.dot(normed, query_weight, preferred_element_type=jnp.float32))
    key_rows = rounded(jnp.dot(normed, key_weight, preferred_element_type=jnp.float32))
    value_rows = rounded(jnp.dot(normed, value_weight, preferred_element_type=jnp.float32))
    out_gate = rounded(jnp.dot(normed, outgate_weight, preferred_element_type=jnp.float32))
    input_pre = jnp.dot(normed, ingate_weight, preferred_element_type=jnp.float32) + ingate_bias
    forget_pre = jnp.dot(normed, forget_weight, preferred_element_type=jnp.float32) + forget_bias
    gated_out, next_memory, next_normalizer, next_stabilizer = memory_step(queries, key_rows, value_rows, out_gate, input_pre, forget_pre, memory_state, normalizer, stabilizer)
    mixed = rounded(jnp.dot(gated_out, output_weight, preferred_element_type=jnp.float32))
    after_mix = rounded(residual + rms_scale(mixed.astype(jnp.float32), postmix_gain))
    after_float = after_mix.astype(jnp.float32)
    expert_input = rms_scale(after_float, prefeed_gain).astype(jnp.bfloat16)
    flat_ids = expert_ids.reshape(-1).astype(jnp.int32)
    one_hot = (flat_ids[:, None] == jnp.arange(EXPERTS, dtype=jnp.int32)[None, :]).astype(jnp.int32)
    earlier = jnp.cumsum(one_hot, axis=0) - one_hot
    slot_ids = lax.optimization_barrier(jnp.sum(earlier * one_hot, axis=1)).astype(jnp.int32)
    token_index = (jnp.arange(SEQS * TOP_K, dtype=jnp.int32) // TOP_K).astype(jnp.int32)
    slot_table = jnp.zeros((EXPERTS, N_EP * CAP), jnp.int32).at[flat_ids, slot_ids].set(token_index)

    def one_expert(inputs):
        rows_index, gate_weight, up_weight, down_weight = inputs
        return expert_rows(expert_input[rows_index], gate_weight, up_weight, down_weight).astype(jnp.bfloat16)
    outputs = lax.map(one_expert, (slot_table, expert_gate, expert_up, expert_down))
    picked = outputs[flat_ids, slot_ids].astype(jnp.float32).reshape(SEQS, TOP_K, D)
    routed = lax.optimization_barrier(jnp.sum(picked * route_weights[:, :, None], axis=1))
    shared_out = expert_rows(expert_input, shared_gate, shared_up, shared_down)
    next_tokens = (after_float + rms_scale(routed + shared_out, postfeed_gain)).astype(jnp.bfloat16)
    return (next_tokens, next_memory, next_normalizer, next_stabilizer)
```

```python
import jax
import jax.numpy as jnp
from jax import lax
from jax.sharding import PartitionSpec as P

epsilon = 1e-06


def rms_scale(values, gain_row):
    return (
        values * lax.rsqrt(jnp.mean(values * values, axis=-1, keepdims=True) + epsilon) * gain_row
    )


def rounded(values):
    return lax.optimization_barrier(values.astype(jnp.bfloat16))


def memory_step(
    queries,
    key_rows,
    value_rows,
    out_gate,
    input_pre,
    forget_pre,
    memory_state,
    normalizer,
    stabilizer,
):
    sequences = queries.shape[0]
    head_count = memory_state.shape[1]
    head_width = memory_state.shape[2]
    query_heads = queries.astype(jnp.float32).reshape(sequences, head_count, head_width)
    key_heads = key_rows.astype(jnp.float32).reshape(
        sequences, head_count, head_width
    ) * head_width ** (-0.5)
    value_heads = value_rows.astype(jnp.float32).reshape(sequences, head_count, head_width)
    carried = jax.nn.log_sigmoid(forget_pre) + stabilizer
    next_stabilizer = jnp.maximum(carried, input_pre)
    keep_old = jnp.exp(carried - next_stabilizer)
    write_new = jnp.exp(input_pre - next_stabilizer)
    local_score = write_new * jnp.sum(query_heads * key_heads, axis=-1)
    read_memory = jnp.einsum(
        "shvk,shk->shv", memory_state, query_heads, precision=lax.Precision.HIGHEST
    )
    numerator = keep_old[..., None] * read_memory + local_score[..., None] * value_heads
    denominator = keep_old * jnp.sum(normalizer * query_heads, axis=-1) + local_score
    memory_read = numerator / jnp.maximum(jnp.abs(denominator), 1.0)[..., None]
    gated_out = (
        jax.nn.sigmoid(out_gate.astype(jnp.float32))
        * memory_read.reshape(sequences, head_count * head_width)
    ).astype(jnp.bfloat16)
    next_memory = (
        keep_old[..., None, None] * memory_state
        + write_new[..., None, None] * value_heads[..., :, None] * key_heads[..., None, :]
    )
    next_normalizer = keep_old[..., None] * normalizer + write_new[..., None] * key_heads
    return (gated_out, next_memory, next_normalizer, next_stabilizer)


def expert_rows(row_block, gate_weight, up_weight, down_weight):
    gate_values = jnp.dot(row_block, gate_weight, preferred_element_type=jnp.float32)
    up_values = jnp.dot(row_block, up_weight, preferred_element_type=jnp.float32)
    inner_rows = (jax.nn.silu(gate_values) * up_values).astype(jnp.bfloat16)
    return jnp.dot(inner_rows, down_weight, preferred_element_type=jnp.float32)


def swap(values, bit):
    devices = lax.axis_size("ep")
    return lax.ppermute(values, "ep", [(i, i ^ bit) for i in range(devices)])


def deal_heads(weights, head_count, place):
    rows, width = weights[0].shape
    head_width = width // head_count
    held = jnp.stack([w.reshape(rows, head_count, head_width) for w in weights], axis=2)
    held = held.reshape(rows, head_count, len(weights) * head_width).swapaxes(0, 1)
    bit = 1
    while bit < head_count:
        side = (place // bit) % 2
        halves = held.reshape(held.shape[0] // 2, 2, *held.shape[1:])
        kept = jnp.where(side == 0, halves[:, 0], halves[:, 1])
        sent = jnp.where(side == 0, halves[:, 1], halves[:, 0])
        came = swap(sent, bit)
        first = jnp.where(side == 0, kept, came)
        second = jnp.where(side == 0, came, kept)
        held = jnp.concatenate([first, second], axis=1)
        bit *= 2
    return held.reshape(rows * head_count, len(weights) * head_width)


def gather_far(weight, place):
    devices = lax.axis_size("ep")
    held = weight[None]
    bit = 4
    while bit < devices:
        side = (place // bit) % 2
        came = swap(held, bit)
        first = jnp.where(side == 0, held, came)
        second = jnp.where(side == 0, came, held)
        held = jnp.concatenate([first, second], axis=0)
        bit *= 2
    return held


def mix_rows(gated_out, far_weight, place):
    blocks, depth, width = far_weight.shape
    sequences = gated_out.shape[0]
    near = swap(gated_out, 1)
    both = jnp.concatenate([gated_out, near], axis=0)
    rows = jnp.concatenate([both, swap(both, 2)], axis=0)
    flat = far_weight.swapaxes(0, 1).reshape(depth, blocks * width)
    out = jnp.dot(rows, flat, preferred_element_type=jnp.float32).astype(jnp.bfloat16)
    out = out.reshape(4, sequences, blocks * width)
    far = swap(out[2:], 2)
    close = swap(jnp.stack([out[1], far[1]]), 1)
    found = (out[0], close[0], far[0], close[1])
    odd = place % 2
    high = (place // 2) % 2
    pick = [jnp.where(odd == 0, found[k], found[k ^ 1]) for k in range(4)]
    pick = [jnp.where(high == 0, pick[k], pick[k ^ 2]) for k in range(4)]
    stacked = jnp.stack([p.reshape(sequences, blocks, width) for p in pick], axis=2)
    return stacked.reshape(sequences, blocks * 4 * width).astype(jnp.float32)


def on_device(
    tokens,
    premix_gain,
    postmix_gain,
    prefeed_gain,
    postfeed_gain,
    query_weight,
    key_weight,
    value_weight,
    outgate_weight,
    ingate_weight,
    forget_weight,
    ingate_bias,
    forget_bias,
    memory_state,
    normalizer,
    stabilizer,
    output_weight,
    expert_ids,
    route_weights,
    expert_gate,
    expert_up,
    expert_down,
    shared_gate,
    shared_up,
    shared_down,
):
    sequences = tokens.shape[0]
    model_width = tokens.shape[1]
    devices = lax.axis_size("ep")
    head_count = memory_state.shape[1]
    head_width = memory_state.shape[2]
    place = lax.axis_index("ep")
    residual = tokens.astype(jnp.float32)
    normed = rms_scale(residual, premix_gain).astype(jnp.bfloat16)
    planes = devices // head_count
    pieces = normed.reshape(sequences, planes, model_width // planes).swapaxes(0, 1)
    pieces = jnp.broadcast_to(
        pieces[:, None], (planes, head_count, sequences, model_width // planes)
    ).reshape(devices, sequences, model_width // planes)
    rows_in = lax.all_to_all(pieces, "ep", split_axis=0, concat_axis=0, tiled=True)
    stacked = deal_heads(
        (query_weight, key_weight, value_weight, outgate_weight), head_count, place
    )
    partial = jnp.dot(
        rows_in.reshape(devices * sequences, model_width // planes),
        stacked,
        preferred_element_type=jnp.float32,
    ).astype(jnp.bfloat16)
    partial = partial.reshape(devices, sequences, 4 * head_width)
    parts = lax.all_to_all(partial, "ep", split_axis=0, concat_axis=0, tiled=True)
    summed = jnp.sum(
        parts.reshape(planes, head_count, sequences, 4, head_width).astype(jnp.float32), axis=0
    )
    projected = summed.transpose(2, 1, 0, 3).reshape(4, sequences, head_count * head_width)
    input_pre = jnp.dot(normed, ingate_weight, preferred_element_type=jnp.float32) + ingate_bias
    forget_pre = jnp.dot(normed, forget_weight, preferred_element_type=jnp.float32) + forget_bias
    gated_out, next_memory, next_normalizer, next_stabilizer = memory_step(
        projected[0],
        projected[1],
        projected[2],
        projected[3],
        input_pre,
        forget_pre,
        memory_state,
        normalizer,
        stabilizer,
    )
    mixed = mix_rows(gated_out, gather_far(output_weight, place), place)
    after_mix = rounded(residual + rms_scale(mixed, postmix_gain))
    after_float = after_mix.astype(jnp.float32)
    expert_input = rms_scale(after_float, prefeed_gain).astype(jnp.bfloat16)
    local_count = expert_gate.shape[0]
    experts_total = local_count * devices
    choose_count = expert_ids.shape[1]
    capacity = min(
        sequences, max(2, 2 * ((sequences * choose_count + experts_total - 1) // experts_total))
    )
    flat_ids = expert_ids.reshape(-1)
    one_hot = (flat_ids[:, None] == jnp.arange(experts_total, dtype=jnp.int32)[None, :]).astype(
        jnp.int32
    )
    earlier = jnp.cumsum(one_hot, axis=0) - one_hot
    slot_ids = jnp.sum(earlier * one_hot, axis=1)
    target = flat_ids * capacity + slot_ids
    pair_hot = (
        target[:, None] == jnp.arange(experts_total * capacity, dtype=jnp.int32)[None, :]
    ).astype(jnp.bfloat16)
    pair_rows = jnp.repeat(expert_input, choose_count, axis=0)
    outgoing = jnp.dot(pair_hot.T, pair_rows, preferred_element_type=jnp.float32).astype(
        jnp.bfloat16
    )
    outgoing = outgoing.reshape(experts_total, capacity, model_width)
    arrived = lax.all_to_all(outgoing, "ep", split_axis=0, concat_axis=0, tiled=True)
    item_count = arrived.shape[1]
    grouped = arrived.reshape(devices, local_count, item_count, model_width)
    gate_values = jnp.einsum(
        "nlid,ldf->nlif", grouped, expert_gate, preferred_element_type=jnp.float32
    )
    up_values = jnp.einsum("nlid,ldf->nlif", grouped, expert_up, preferred_element_type=jnp.float32)
    inner_rows = (jax.nn.silu(gate_values) * up_values).astype(jnp.bfloat16)
    answer = jnp.einsum(
        "nlif,lfd->nlid", inner_rows, expert_down, preferred_element_type=jnp.float32
    ).astype(jnp.bfloat16)
    answered = answer.reshape(devices * local_count, item_count, model_width)
    returned = lax.all_to_all(answered, "ep", split_axis=0, concat_axis=0, tiled=True)
    picked = jnp.dot(
        pair_hot,
        returned.reshape(experts_total * capacity, model_width),
        preferred_element_type=jnp.float32,
    )
    routed = jnp.sum(
        picked.reshape(sequences, choose_count, model_width) * route_weights[:, :, None], axis=1
    )
    shared_out = expert_rows(expert_input, shared_gate, shared_up, shared_down)
    next_tokens = (after_float + rms_scale(routed + shared_out, postfeed_gain)).astype(jnp.bfloat16)
    return (next_tokens, next_memory, next_normalizer, next_stabilizer)


def solution(mesh):
    in_specs = (
        P("ep", None),
        P(),
        P(),
        P(),
        P(),
        P("ep", None),
        P("ep", None),
        P("ep", None),
        P("ep", None),
        P(),
        P(),
        P(),
        P(),
        P("ep", None, None, None),
        P("ep", None, None),
        P("ep", None),
        P(None, "ep"),
        P("ep", None),
        P("ep", None),
        P("ep", None, None),
        P("ep", None, None),
        P("ep", None, None),
        P(),
        P(),
        P(),
    )
    out_specs = (P("ep", None), P("ep", None, None, None), P("ep", None, None), P("ep", None))
    return jax.shard_map(
        on_device, mesh=mesh, in_specs=in_specs, out_specs=out_specs, check_vma=False
    )
```

```python
import functools
import jax
import jax.numpy as jnp
from jax import lax
from jax.experimental import pallas as pl
from jax.experimental.pallas import tpu as pltpu
from jax.sharding import PartitionSpec as P

epsilon = 1e-06
CORE = 1
WIDE, HALF = jnp.float32, jnp.bfloat16


def rms_scale(values, gain_row):
    return (
        values * lax.rsqrt(jnp.mean(values * values, axis=-1, keepdims=True) + epsilon) * gain_row
    )


def swap(values, bit):
    devices = lax.axis_size("ep")
    return lax.ppermute(values, "ep", [(i, i ^ bit) for i in range(devices)])


def exchange(values, groups=None):
    return lax.all_to_all(
        values, "ep", split_axis=0, concat_axis=0, tiled=True, axis_index_groups=groups
    )


SPACES = {"v": pltpu.VMEM, "h": pltpu.HBM, "s": pltpu.SMEM}


def local_call(body, outs, args, spaces=None, scratch=(), limit=16):
    spaces = spaces or "v" * len(args)
    args = [
        pltpu.with_memory_space_constraint(arg, SPACES[space]) if space != "s" else arg
        for arg, space in zip(args, spaces)
    ]
    return pl.pallas_call(
        body,
        out_shape=[SPACES[space](shape, kind) for shape, kind, space in outs],
        in_specs=[pl.BlockSpec(memory_space=SPACES[space]) for space in spaces],
        out_specs=[pl.BlockSpec(memory_space=pltpu.VMEM)] * len(outs),
        scratch_shapes=list(scratch),
        compiler_params=pltpu.CompilerParams(vmem_limit_bytes=limit * 2**20),
    )(*args)


def fetch(pairs, done):
    copies = [
        pltpu.make_async_copy(source, target, done.at[number])
        for number, (source, target) in enumerate(pairs)
    ]
    for copy in copies:
        copy.start()
    for copy in copies:
        copy.wait()


def start_kernel(at_ref, tokens_ref, gain_ref, *refs, planes):
    weights, outs, (scale_ref, done) = refs[:4], refs[4:-2], refs[-2:]
    kept_ref, sent_ref, held_ref, normed_ref, pieces_ref = outs
    loads = [
        pltpu.make_async_copy(source, target, done.at[number])
        for number, (source, target) in enumerate([(tokens_ref, held_ref), (gain_ref, scale_ref)])
    ]
    for load in loads:
        load.start()

    def place(kept, sent):
        pairs = [(weight, kept_ref.at[number]) for number, weight in enumerate(kept)]
        pairs += [(weight, sent_ref.at[number]) for number, weight in enumerate(sent)]
        for number, (source, target) in enumerate(pairs):
            pltpu.make_async_copy(source, target, done.at[2 + number]).start()

    pl.when(at_ref[0] == 0)(lambda: place(weights[:2], weights[2:]))
    pl.when(at_ref[0] != 0)(lambda: place(weights[2:], weights[:2]))
    for load in loads:
        load.wait()
    normed = rms_scale(held_ref[...].astype(WIDE), scale_ref[...]).astype(HALF)
    normed_ref[...] = normed
    width = normed.shape[1] // planes
    copies = pieces_ref.shape[0] // planes
    for plane in range(planes):
        piece = normed[:, plane * width : (plane + 1) * width]
        for copy in range(copies):
            pieces_ref[plane * copies + copy] = piece
    for number in range(2):
        for side, target in enumerate((kept_ref, sent_ref)):
            source = weights[number]
            pltpu.make_async_copy(source, target.at[number], done.at[2 + 2 * side + number]).wait()


def deal_kernel(at_ref, kept_ref, came_ref, *outs):
    core, chip = at_ref[0], at_ref[1]
    count, rows, _ = kept_ref.shape
    lanes = outs[0].shape[1] // count
    mine = pl.multiple_of(core * rows, rows)
    other = pl.multiple_of((1 - core) * rows, rows)
    for turn, out in enumerate(outs):
        start = pl.multiple_of((chip ^ turn) * lanes, lanes)
        for number in range(count):
            across = slice(number * lanes, (number + 1) * lanes)
            out[pl.ds(mine, rows), across] = kept_ref[number, :, pl.ds(start, lanes)]
            out[pl.ds(other, rows), across] = came_ref[number, :, pl.ds(start, lanes)]


def prepare_kernel(
    normed_ref, *refs, fold, capacity
):
    sources, outs, held, done = refs[:11], refs[11:20], refs[20:-1], refs[-1]
    keep_ref, write_ref, next_ref, hot_ref, pick_ref = outs[:5]
    fetch(list(zip(sources, outs[5:] + held)), done)
    ingate_ref, forget_ref, ingate_bias, forget_bias, stabilizer_ref, ids_ref, route_ref = held
    normed = normed_ref[...]
    dims = (((1,), (1,)), ((), ()))
    input_pre = lax.dot_general(normed, ingate_ref[...], dims, preferred_element_type=WIDE)
    input_pre = input_pre + ingate_bias[...]
    forget_pre = lax.dot_general(normed, forget_ref[...], dims, preferred_element_type=WIDE)
    forget_pre = forget_pre + forget_bias[...]
    carried = jax.nn.log_sigmoid(forget_pre) + stabilizer_ref[...]
    following = jnp.maximum(carried, input_pre)
    next_ref[...] = following
    keep_ref[...] = jnp.exp(carried - following)
    write_ref[...] = jnp.exp(input_pre - following)

    sequences, choose_count = ids_ref.shape
    slots = hot_ref.shape[1]
    slot = lax.broadcasted_iota(jnp.int32, (sequences, slots), 1)
    order = lax.broadcasted_iota(jnp.int32, (sequences, slots), 0)
    expert = slot // (fold * capacity)
    named = jnp.zeros((sequences, slots), WIDE)
    share = jnp.zeros((sequences, slots), WIDE)
    for choice in range(choose_count):
        match = ids_ref[:, choice : choice + 1] == expert
        named = jnp.where(match, 1.0, named)
        share = jnp.where(match, route_ref[:, choice : choice + 1], share)
    rank = jnp.zeros((sequences, slots), WIDE)
    for earlier in range(sequences - 1):
        rank = rank + jnp.where(order > earlier, named[earlier : earlier + 1], 0.0)
    taken = (named > 0.0) & (rank == (slot % capacity).astype(WIDE))
    part_of = (slot // capacity) % fold
    high = share.astype(HALF).astype(WIDE)
    low = share - high
    for part in range(fold):
        here = taken & (part_of == part)
        rows = slice(part * sequences, (part + 1) * sequences)
        hot_ref[rows] = jnp.where(here, 1.0, 0.0).astype(HALF)
        start = 2 * part * sequences
        pick_ref[start : start + sequences] = jnp.where(here, high, 0.0).astype(HALF)
        pick_ref[start + sequences : start + 2 * sequences] = jnp.where(here, low, 0.0).astype(HALF)


def project_kernel(at_ref, rows_ref, *refs):
    blocks, out_ref, held_ref = refs[:-2], refs[-2], refs[-1]
    chip = at_ref[1]
    depth = blocks[0].shape[0]
    for turn, block in enumerate(blocks):
        start = pl.multiple_of((chip ^ turn) * depth, depth)
        held_ref[pl.ds(start, depth), :] = block[...]
    out_ref[...] = jnp.dot(
        rows_ref[...], held_ref[...], preferred_element_type=WIDE
    ).astype(HALF)


def hold_kernel(after_ref, memory_ref, held_ref, done):
    load = pltpu.make_async_copy(memory_ref.at[pl.ds(0, held_ref.shape[0])], held_ref, done)
    load.start()
    load.wait()


def read_kernel(
    parts_ref,
    keep_ref,
    write_ref,
    normalizer_ref,
    early_ref,
    memory_ref,
    gated_ref,
    keys_ref,
    values_ref,
    late_ref,
    done,
):
    early = early_ref.shape[0]
    loads = [
        pltpu.make_async_copy(memory_ref.at[early + at], late_ref.at[at], done.at[at])
        for at in range(late_ref.shape[0])
    ]
    for load in loads:
        load.start()
    copies, sequences, _ = gated_ref.shape
    heads, width = memory_ref.shape[1], memory_ref.shape[3]
    planes = parts_ref.shape[0] // heads
    row = lax.broadcasted_iota(jnp.int32, (sequences, width), 0)
    pieces, asked = [], []
    for head in range(heads):
        first = head % 2 * width
        found = []
        for core in range(2):
            for start in (first, first + 2 * width):
                total = 0.0
                for plane in range(planes):
                    part = parts_ref[plane * heads + head // 2 * 2 + core]
                    total = total + part[:, start : start + width].astype(WIDE)
                found.append(total)
        found[1] = found[1] * width ** (-0.5)
        keys_ref[head] = found[1]
        values_ref[head] = found[2]
        pieces.append(found)
        high = found[0].astype(HALF)
        low = (found[0] - high.astype(WIDE)).astype(HALF)
        both = jnp.concatenate([high, low], axis=0)
        asked.append(jnp.concatenate([both, both], axis=1))
    dims = (((1,), (1,)), ((), ()))
    reads = [jnp.zeros((sequences, width), WIDE)] * heads
    for sequence in range(sequences):
        if sequence >= early:
            loads[sequence - early].wait()
        for first in range(0, heads, 2):
            held = []
            for head in (first, first + 1):
                if sequence < early:
                    memory = early_ref[sequence, head]
                else:
                    memory = late_ref[sequence - early, head]
                upper = memory.astype(HALF)
                lower = (memory - upper.astype(WIDE)).astype(HALF)
                held.append(jnp.concatenate([upper, lower], axis=1))
            answer = lax.dot_general(
                jnp.concatenate([asked[first], asked[first + 1]], axis=0),
                jnp.concatenate(held, axis=0),
                dims,
                preferred_element_type=WIDE,
            )
            for side in range(2):
                start = 2 * side * sequences
                mine = answer[start : start + 2 * sequences, side * width : (side + 1) * width]
                mine = mine[:sequences] + mine[sequences:]
                head = first + side
                reads[head] = jnp.where(row == sequence, mine, reads[head])
    for head in range(heads):
        queries, keys, values, gate = pieces[head]
        keep = keep_ref[:, head : head + 1]
        score = write_ref[:, head : head + 1] * jnp.sum(queries * keys, axis=-1, keepdims=True)
        below = (
            keep * jnp.sum(normalizer_ref[:, head] * queries, axis=-1, keepdims=True) + score
        )
        answer = (keep * reads[head] + score * values) / jnp.maximum(jnp.abs(below), 1.0)
        gated = (jax.nn.sigmoid(gate) * answer).astype(HALF)
        for copy in range(copies):
            gated_ref[copy, :, head * width : (head + 1) * width] = gated


def stack_kernel(at_ref, *refs):
    out_ref = refs[-1]
    core, chip = at_ref[0], at_ref[1]
    blocks = refs[:-1]
    mine, other = blocks[: len(blocks) // 2], blocks[len(blocks) // 2 :]
    turn = 0
    for ours, theirs in zip(mine, other):
        count, rows, _ = ours.shape
        for at in range(count):
            start = (chip ^ turn) * 2 * rows
            out_ref[pl.ds(pl.multiple_of(start + core * rows, rows), rows), :] = ours[at]
            out_ref[pl.ds(pl.multiple_of(start + (1 - core) * rows, rows), rows), :] = theirs[at]
            turn += 1


def mix_kernel(rows_ref, weight_ref, out_ref):
    out_ref[...] = lax.dot_general(
        rows_ref[...], weight_ref[...], (((1,), (1,)), ((), ())), preferred_element_type=WIDE
    ).astype(HALF)


def send_kernel(
    mixed_ref, tokens_ref, postmix_ref, prefeed_ref, hot_ref, after_ref, input_ref, out_ref
):
    mixed = jnp.concatenate([mixed_ref[i] for i in range(mixed_ref.shape[0])], axis=1)
    residual = tokens_ref[...].astype(WIDE)
    after = (residual + rms_scale(mixed.astype(WIDE), postmix_ref[...])).astype(HALF)
    after_ref[...] = after
    given = rms_scale(after.astype(WIDE), prefeed_ref[...])
    input_ref[...] = given.astype(HALF)
    width = out_ref.shape[1]
    folded = jnp.concatenate(
        [given[:, at : at + width] for at in range(0, given.shape[1], width)], axis=0
    ).astype(HALF)
    dims = (((0,), (0,)), ((), ()))
    out_ref[...] = lax.dot_general(
        hot_ref[...], folded, dims, preferred_element_type=WIDE
    ).astype(HALF)


def turned(values, by):
    by = by % values.shape[1]
    return pltpu.roll(values, by, 1) if by else values


def hold_gate_kernel(after_ref, weight_ref, held_ref, done):
    load = pltpu.make_async_copy(weight_ref, held_ref, done)
    load.start()
    load.wait()


def expert_kernel(came_ref, gate_ref, up_ref, down_ref, out_ref, held_up, held_down, done):
    groups, fold, tall, width = came_ref.shape
    capacity = tall // fold
    spans = [pl.ds(part * width, width) for part in range(fold)]
    loads = [(up_ref.at[span], held_up.at[span]) for span in spans]
    loads += [(down_ref.at[:, span], held_down.at[:, span]) for span in spans]
    loads = [
        pltpu.make_async_copy(source, target, done.at[number])
        for number, (source, target) in enumerate(loads)
    ]
    for load in loads:
        load.start()
    area = lax.broadcasted_iota(jnp.int32, (groups, tall, width), 1) // capacity
    came = [came_ref[:, at].astype(WIDE) for at in range(fold)]
    gates, ups, given = 0.0, 0.0, []
    for part in range(fold):
        for at in range(fold):
            piece = turned(came[at], (at - part) * capacity)
            rows = piece if at == 0 else jnp.where(area == at, piece, rows)
        given.append(rows.reshape(groups * tall, width).astype(HALF))
        gates = gates + jnp.dot(
            given[part], gate_ref[part * width : (part + 1) * width], preferred_element_type=WIDE
        )
    for part in range(fold):
        loads[part].wait()
        ups = ups + jnp.dot(
            given[part], held_up[part * width : (part + 1) * width], preferred_element_type=WIDE
        )
    hidden = (jax.nn.silu(gates) * ups).astype(HALF)
    answers = []
    for part in range(fold):
        loads[fold + part].wait()
        answer = jnp.dot(
            hidden, held_down[:, part * width : (part + 1) * width], preferred_element_type=WIDE
        )
        answers.append(answer.reshape(groups, tall, width))
    for at in range(fold):
        for part in range(fold):
            piece = turned(answers[part], (part - at) * capacity)
            packed = piece if part == 0 else jnp.where(area == part, piece, packed)
        out_ref[:, at] = packed.astype(HALF)


def shared_kernel(input_ref, gate_ref, up_ref, down_ref, out_ref):
    rows = input_ref[...]
    gates = jnp.dot(rows, gate_ref[...], preferred_element_type=WIDE)
    ups = jnp.dot(rows, up_ref[...], preferred_element_type=WIDE)
    hidden = (jax.nn.silu(gates) * ups).astype(HALF)
    out_ref[...] = jnp.dot(hidden, down_ref[...], preferred_element_type=WIDE)


def final_kernel(back_ref, weights_ref, shared_ref, after_ref, gain_ref, out_ref):
    sequences = out_ref.shape[0]
    picked = jnp.dot(weights_ref[...], back_ref[...], preferred_element_type=WIDE)
    step = 2 * sequences
    routed = jnp.concatenate(
        [
            picked[at : at + sequences] + picked[at + sequences : at + step]
            for at in range(0, picked.shape[0], step)
        ],
        axis=1,
    )
    out_ref[...] = (
        after_ref[...].astype(WIDE) + rms_scale(routed + shared_ref[...], gain_ref[...])
    ).astype(HALF)


def on_device(
    tokens,
    premix_gain,
    postmix_gain,
    prefeed_gain,
    postfeed_gain,
    query_weight,
    key_weight,
    value_weight,
    outgate_weight,
    ingate_weight,
    forget_weight,
    ingate_bias,
    forget_bias,
    memory_state,
    normalizer,
    stabilizer,
    output_weight,
    expert_ids,
    route_weights,
    expert_gate,
    expert_up,
    expert_down,
    shared_gate,
    shared_up,
    shared_down,
):
    sequences, model_width = tokens.shape
    devices = lax.axis_size("ep")
    heads, width = memory_state.shape[1], memory_state.shape[3]
    planes = devices // heads
    chips = heads // 2
    place = lax.axis_index("ep")
    at = jnp.stack([place % 2, (place // 2) % chips]).astype(jnp.int32)

    rows = query_weight.shape[0]
    piece_width = model_width // planes
    local_count = expert_gate.shape[0]
    experts_total = local_count * devices
    choose_count = expert_ids.shape[1]
    capacity = min(
        sequences, max(2, 2 * ((sequences * choose_count + experts_total - 1) // experts_total))
    )
    fold = max(1, 8 // capacity)
    tall = fold * capacity
    slot_count = experts_total * tall
    slot_width = model_width // fold

    kept, sent, held_tokens, normed, pieces = local_call(
        functools.partial(start_kernel, planes=planes),
        [
            ((2, *query_weight.shape), HALF, "v"),
            ((2, *query_weight.shape), HALF, "v"),
            ((sequences, model_width), HALF, "v"),
            ((sequences, model_width), HALF, "v"),
            ((devices, sequences, piece_width), HALF, "h"),
        ],
        (at, tokens, premix_gain[None], query_weight, key_weight, value_weight, outgate_weight),
        "shhhhhh",
        scratch=[pltpu.VMEM((1, model_width), WIDE), pltpu.SemaphoreType.DMA((6,))],
    )
    came = swap(sent, CORE)
    rows_in = exchange(pieces)
    dealt = local_call(
        deal_kernel, [((2 * rows, 4 * width), HALF, "v")] * chips, (at, kept, came), "svv"
    )
    blocks = [dealt[0]] + [swap(dealt[turn], CORE * 2 * turn) for turn in range(1, chips)]

    own_out = output_weight.T[None]
    near_out = [own_out] + [swap(own_out, CORE * 2 * turn) for turn in range(1, chips)]
    far_out = [swap(block, CORE) for block in near_out]
    (mix_weight,) = local_call(
        stack_kernel,
        [((piece_width, heads * width), HALF, "v")],
        (at, *near_out, *far_out),
        "s" + "v" * 2 * chips,
    )

    small = (
        ingate_weight.T,
        forget_weight.T,
        ingate_bias[None],
        forget_bias[None],
        stabilizer,
        expert_ids,
        route_weights,
    )
    keep_old, write_new, next_stabilizer, hot, pick, *gains, held_normalizer = local_call(
        functools.partial(prepare_kernel, fold=fold, capacity=capacity),
        [
            ((sequences, heads), WIDE, "v"),
            ((sequences, heads), WIDE, "v"),
            ((sequences, heads), WIDE, "h"),
            ((fold * sequences, slot_count), HALF, "v"),
            ((2 * fold * sequences, slot_count), HALF, "v"),
            ((1, model_width), WIDE, "v"),
            ((1, model_width), WIDE, "v"),
            ((1, model_width), WIDE, "v"),
            (normalizer.shape, WIDE, "v"),
        ],
        (normed, postmix_gain[None], prefeed_gain[None], postfeed_gain[None], normalizer, *small),
        "v" + "h" * 11,
        scratch=[
            *(pltpu.VMEM(array.shape, array.dtype) for array in small),
            pltpu.SemaphoreType.DMA((11,)),
        ],
    )

    (partial,) = local_call(
        project_kernel,
        [((devices * sequences, 4 * width), HALF, "h")],
        (at, rows_in.reshape(devices * sequences, piece_width), *blocks),
        "sv" + "v" * chips,
        scratch=[pltpu.VMEM((piece_width, 4 * width), HALF)],
    )
    partial = partial.reshape(devices, sequences, 4 * width)
    parts = exchange(partial)
    early = 3 * sequences // 8
    (early_memory,) = local_call(
        hold_kernel,
        [((early, *memory_state.shape[1:]), WIDE, "v")],
        (partial, memory_state),
        "hh",
        scratch=[pltpu.SemaphoreType.DMA],
    )
    gated, keys, values = local_call(
        read_kernel,
        [
            ((planes, sequences, heads * width), HALF, "h"),
            ((heads, sequences, width), WIDE, "v"),
            ((heads, sequences, width), WIDE, "v"),
        ],
        (parts, keep_old, write_new, held_normalizer, early_memory, memory_state),
        "vvvvvh",
        scratch=[
            pltpu.VMEM((sequences - early, *memory_state.shape[1:]), WIDE),
            pltpu.SemaphoreType.DMA((sequences - early,)),
        ],
    )
    lines = [[low + heads * plane for plane in range(planes)] for low in range(heads)]
    gathered = exchange(gated, lines)
    (mixed,) = local_call(
        mix_kernel,
        [((planes * sequences, piece_width), HALF, "h")],
        (gathered.reshape(planes * sequences, heads * width), mix_weight),
    )
    mixed = exchange(mixed.reshape(planes, sequences, piece_width), lines)
    after_mix, expert_input, outgoing = local_call(
        send_kernel,
        [
            ((sequences, model_width), HALF, "v"),
            ((sequences, model_width), HALF, "v"),
            ((slot_count, slot_width), HALF, "h"),
        ],
        (mixed, held_tokens, gains[0], gains[1], hot),
    )
    outgoing = outgoing.reshape(experts_total, tall, slot_width)
    arrived = exchange(outgoing)
    arrived = arrived.reshape(devices, local_count, tall, slot_width)
    answers = []
    for expert in range(local_count):
        (held_gate,) = local_call(
            hold_gate_kernel,
            [(expert_gate.shape[1:], HALF, "v")],
            (after_mix, expert_gate[expert]),
            "vh",
            scratch=[pltpu.SemaphoreType.DMA],
        )
        (answer,) = local_call(
            expert_kernel,
            [((devices // fold, fold, tall, slot_width), HALF, "h")],
            (
                arrived[:, expert].reshape(devices // fold, fold, tall, slot_width),
                held_gate,
                expert_up[expert],
                expert_down[expert],
            ),
            "vvhh",
            scratch=[
                pltpu.VMEM(expert_up.shape[1:], HALF),
                pltpu.VMEM(expert_down.shape[1:], HALF),
                pltpu.SemaphoreType.DMA((2 * fold,)),
            ],
        )
        answers.append(answer.reshape(devices, tall, slot_width))
    answered = jnp.stack(answers, axis=1).reshape(experts_total, tall, slot_width)
    returned = exchange(answered)

    (shared_out,) = local_call(
        shared_kernel,
        [((sequences, model_width), WIDE, "v")],
        (expert_input, shared_gate, shared_up, shared_down),
    )
    key_rows, value_rows = keys.swapaxes(0, 1), values.swapaxes(0, 1)
    next_memory = (
        keep_old[..., None, None] * memory_state
        + write_new[..., None, None] * value_rows[..., :, None] * key_rows[..., None, :]
    )
    next_normalizer = keep_old[..., None] * normalizer + write_new[..., None] * key_rows
    (next_tokens,) = local_call(
        final_kernel,
        [((sequences, model_width), HALF, "h")],
        (returned.reshape(slot_count, slot_width), pick, shared_out, after_mix, gains[2]),
    )
    return (next_tokens, next_memory, next_normalizer, next_stabilizer)


def solution(mesh):
    in_specs = (
        P("ep", None),
        P(),
        P(),
        P(),
        P(),
        P("ep", None),
        P("ep", None),
        P("ep", None),
        P("ep", None),
        P(),
        P(),
        P(),
        P(),
        P("ep", None, None, None),
        P("ep", None, None),
        P("ep", None),
        P(None, "ep"),
        P("ep", None),
        P("ep", None),
        P("ep", None, None),
        P("ep", None, None),
        P("ep", None, None),
        P(),
        P(),
        P(),
    )
    out_specs = (P("ep", None), P("ep", None, None, None), P("ep", None, None), P("ep", None))

    return jax.shard_map(
        on_device, mesh=mesh, in_specs=in_specs, out_specs=out_specs, check_vma=False
    )
```

```python
import functools
import jax
import jax.numpy as jnp
from jax import lax
from jax.experimental import pallas as pl
from jax.experimental.pallas import tpu as pltpu
from jax.sharding import PartitionSpec as P

epsilon = 1e-06
CORE = 1
WIDE, HALF = jnp.float32, jnp.bfloat16


def rms_scale(values, gain_row):
    return (
        values * lax.rsqrt(jnp.mean(values * values, axis=-1, keepdims=True) + epsilon) * gain_row
    )


def swap(values, bit):
    devices = lax.axis_size("ep")
    return lax.ppermute(values, "ep", [(i, i ^ bit) for i in range(devices)])


def exchange(values, groups=None):
    return lax.all_to_all(
        values, "ep", split_axis=0, concat_axis=0, tiled=True, axis_index_groups=groups
    )


SPACES = {"v": pltpu.VMEM, "h": pltpu.HBM, "s": pltpu.SMEM}


def local_call(body, outs, args, spaces=None, scratch=(), limit=16):
    spaces = spaces or "v" * len(args)
    args = [
        pltpu.with_memory_space_constraint(arg, SPACES[space]) if space != "s" else arg
        for arg, space in zip(args, spaces)
    ]
    return pl.pallas_call(
        body,
        out_shape=[SPACES[space](shape, kind) for shape, kind, space in outs],
        in_specs=[pl.BlockSpec(memory_space=SPACES[space]) for space in spaces],
        out_specs=[pl.BlockSpec(memory_space=pltpu.VMEM)] * len(outs),
        scratch_shapes=list(scratch),
        compiler_params=pltpu.CompilerParams(vmem_limit_bytes=limit * 2**20),
    )(*args)


def fetch(pairs, done):
    copies = [
        pltpu.make_async_copy(source, target, done.at[number])
        for number, (source, target) in enumerate(pairs)
    ]
    for copy in copies:
        copy.start()
    for copy in copies:
        copy.wait()


def start_kernel(at_ref, tokens_ref, gain_ref, *refs, planes):
    weights, outs, (scale_ref, done) = refs[:4], refs[4:-2], refs[-2:]
    kept_ref, sent_ref, held_ref, normed_ref, pieces_ref = outs
    loads = [
        pltpu.make_async_copy(source, target, done.at[number])
        for number, (source, target) in enumerate([(tokens_ref, held_ref), (gain_ref, scale_ref)])
    ]
    for load in loads:
        load.start()

    def place(kept, sent):
        pairs = [(weight, kept_ref.at[number]) for number, weight in enumerate(kept)]
        pairs += [(weight, sent_ref.at[number]) for number, weight in enumerate(sent)]
        for number, (source, target) in enumerate(pairs):
            pltpu.make_async_copy(source, target, done.at[2 + number]).start()

    pl.when(at_ref[0] == 0)(lambda: place(weights[:2], weights[2:]))
    pl.when(at_ref[0] != 0)(lambda: place(weights[2:], weights[:2]))
    for load in loads:
        load.wait()
    normed = rms_scale(held_ref[...].astype(WIDE), scale_ref[...]).astype(HALF)
    normed_ref[...] = normed
    width = normed.shape[1] // planes
    copies = pieces_ref.shape[0] // planes
    for plane in range(planes):
        piece = normed[:, plane * width : (plane + 1) * width]
        for copy in range(copies):
            pieces_ref[plane * copies + copy] = piece
    for number in range(2):
        for side, target in enumerate((kept_ref, sent_ref)):
            source = weights[number]
            pltpu.make_async_copy(source, target.at[number], done.at[2 + 2 * side + number]).wait()


def deal_kernel(at_ref, kept_ref, came_ref, *outs):
    core, chip = at_ref[0], at_ref[1]
    count, rows, _ = kept_ref.shape
    lanes = outs[0].shape[1] // count
    mine = pl.multiple_of(core * rows, rows)
    other = pl.multiple_of((1 - core) * rows, rows)
    for turn, out in enumerate(outs):
        start = pl.multiple_of((chip ^ turn) * lanes, lanes)
        for number in range(count):
            across = slice(number * lanes, (number + 1) * lanes)
            out[pl.ds(mine, rows), across] = kept_ref[number, :, pl.ds(start, lanes)]
            out[pl.ds(other, rows), across] = came_ref[number, :, pl.ds(start, lanes)]


def prepare_kernel(
    normed_ref, *refs, fold, capacity
):
    sources, outs, held, done = refs[:11], refs[11:20], refs[20:-1], refs[-1]
    keep_ref, write_ref, next_ref, hot_ref, pick_ref = outs[:5]
    fetch(list(zip(sources, outs[5:] + held)), done)
    ingate_ref, forget_ref, ingate_bias, forget_bias, stabilizer_ref, ids_ref, route_ref = held
    normed = normed_ref[...]
    dims = (((1,), (1,)), ((), ()))
    input_pre = lax.dot_general(normed, ingate_ref[...], dims, preferred_element_type=WIDE)
    input_pre = input_pre + ingate_bias[...]
    forget_pre = lax.dot_general(normed, forget_ref[...], dims, preferred_element_type=WIDE)
    forget_pre = forget_pre + forget_bias[...]
    carried = jax.nn.log_sigmoid(forget_pre) + stabilizer_ref[...]
    following = jnp.maximum(carried, input_pre)
    next_ref[...] = following
    keep_ref[...] = jnp.exp(carried - following)
    write_ref[...] = jnp.exp(input_pre - following)

    sequences, choose_count = ids_ref.shape
    slots = hot_ref.shape[1]
    slot = lax.broadcasted_iota(jnp.int32, (sequences, slots), 1)
    order = lax.broadcasted_iota(jnp.int32, (sequences, slots), 0)
    expert = slot // (fold * capacity)
    named = jnp.zeros((sequences, slots), WIDE)
    share = jnp.zeros((sequences, slots), WIDE)
    for choice in range(choose_count):
        match = ids_ref[:, choice : choice + 1] == expert
        named = jnp.where(match, 1.0, named)
        share = jnp.where(match, route_ref[:, choice : choice + 1], share)
    rank = jnp.zeros((sequences, slots), WIDE)
    for earlier in range(sequences - 1):
        rank = rank + jnp.where(order > earlier, named[earlier : earlier + 1], 0.0)
    taken = (named > 0.0) & (rank == (slot % capacity).astype(WIDE))
    part_of = (slot // capacity) % fold
    high = share.astype(HALF).astype(WIDE)
    low = share - high
    for part in range(fold):
        here = taken & (part_of == part)
        rows = slice(part * sequences, (part + 1) * sequences)
        hot_ref[rows] = jnp.where(here, 1.0, 0.0).astype(HALF)
        start = 2 * part * sequences
        pick_ref[start : start + sequences] = jnp.where(here, high, 0.0).astype(HALF)
        pick_ref[start + sequences : start + 2 * sequences] = jnp.where(here, low, 0.0).astype(HALF)


def project_kernel(at_ref, rows_ref, *refs):
    blocks, out_ref, held_ref = refs[:-2], refs[-2], refs[-1]
    chip = at_ref[1]
    depth = blocks[0].shape[0]
    for turn, block in enumerate(blocks):
        start = pl.multiple_of((chip ^ turn) * depth, depth)
        held_ref[pl.ds(start, depth), :] = block[...]
    out_ref[...] = jnp.dot(
        rows_ref[...], held_ref[...], preferred_element_type=WIDE
    ).astype(HALF)


def hold_kernel(after_ref, memory_ref, held_ref, done):
    load = pltpu.make_async_copy(memory_ref.at[pl.ds(0, held_ref.shape[0])], held_ref, done)
    load.start()
    load.wait()


def read_kernel(
    parts_ref,
    keep_ref,
    write_ref,
    normalizer_ref,
    early_ref,
    memory_ref,
    gated_ref,
    keys_ref,
    values_ref,
    late_ref,
    done,
):
    early = early_ref.shape[0]
    loads = [
        pltpu.make_async_copy(memory_ref.at[early + at], late_ref.at[at], done.at[at])
        for at in range(late_ref.shape[0])
    ]
    for load in loads:
        load.start()
    copies, sequences, _ = gated_ref.shape
    heads, width = memory_ref.shape[1], memory_ref.shape[3]
    planes = parts_ref.shape[0] // heads
    row = lax.broadcasted_iota(jnp.int32, (sequences, width), 0)
    pieces, asked = [], []
    for head in range(heads):
        first = head % 2 * width
        found = []
        for core in range(2):
            for start in (first, first + 2 * width):
                total = 0.0
                for plane in range(planes):
                    part = parts_ref[plane * heads + head // 2 * 2 + core]
                    total = total + part[:, start : start + width].astype(WIDE)
                found.append(total)
        found[1] = found[1] * width ** (-0.5)
        keys_ref[head] = found[1]
        values_ref[head] = found[2]
        pieces.append(found)
        high = found[0].astype(HALF)
        low = (found[0] - high.astype(WIDE)).astype(HALF)
        both = jnp.concatenate([high, low], axis=0)
        asked.append(jnp.concatenate([both, both], axis=1))
    dims = (((1,), (1,)), ((), ()))
    reads = [jnp.zeros((sequences, width), WIDE)] * heads
    for sequence in range(sequences):
        if sequence >= early:
            loads[sequence - early].wait()
        for first in range(0, heads, 2):
            held = []
            for head in (first, first + 1):
                if sequence < early:
                    memory = early_ref[sequence, head]
                else:
                    memory = late_ref[sequence - early, head]
                upper = memory.astype(HALF)
                lower = (memory - upper.astype(WIDE)).astype(HALF)
                held.append(jnp.concatenate([upper, lower], axis=1))
            answer = lax.dot_general(
                jnp.concatenate([asked[first], asked[first + 1]], axis=0),
                jnp.concatenate(held, axis=0),
                dims,
                preferred_element_type=WIDE,
            )
            for side in range(2):
                start = 2 * side * sequences
                mine = answer[start : start + 2 * sequences, side * width : (side + 1) * width]
                mine = mine[:sequences] + mine[sequences:]
                head = first + side
                reads[head] = jnp.where(row == sequence, mine, reads[head])
    for head in range(heads):
        queries, keys, values, gate = pieces[head]
        keep = keep_ref[:, head : head + 1]
        score = write_ref[:, head : head + 1] * jnp.sum(queries * keys, axis=-1, keepdims=True)
        below = (
            keep * jnp.sum(normalizer_ref[:, head] * queries, axis=-1, keepdims=True) + score
        )
        answer = (keep * reads[head] + score * values) / jnp.maximum(jnp.abs(below), 1.0)
        gated = (jax.nn.sigmoid(gate) * answer).astype(HALF)
        for copy in range(copies):
            gated_ref[copy, :, head * width : (head + 1) * width] = gated


def merge_kernel(*refs):
    out_ref = refs[-1]
    for number, block in enumerate(refs[:-1]):
        out_ref[number] = block[0]


def stack_kernel(at_ref, *refs):
    blocks, out_ref = refs[:-1], refs[-1]
    core, chip, side = at_ref[0], at_ref[1], at_ref[2]
    chips = len(blocks) // 2
    count, rows, _ = blocks[0].shape
    for turn in range(chips):
        for number in range(count):
            start = ((side ^ number) * chips + (chip ^ turn)) * 2 * rows
            for block, half in ((blocks[turn], core), (blocks[chips + turn], 1 - core)):
                place = pl.ds(pl.multiple_of(start + half * rows, rows), rows)
                out_ref[place, :] = block[number]


def mix_kernel(*refs):
    rows = jnp.concatenate([ref[...] for ref in refs[:-2]], axis=0)
    refs[-1][...] = lax.dot_general(
        rows, refs[-2][...], (((1,), (1,)), ((), ())), preferred_element_type=WIDE
    ).astype(HALF)


def send_kernel(at_ref, *refs, pieces):
    mixed, refs = [piece[...].astype(WIDE) for piece in refs[:pieces]], refs[pieces:]
    homes = (len(refs) - 5) // 2
    tokens, hots, refs = refs[:homes], refs[homes : 2 * homes], refs[2 * homes :]
    postmix_ref, prefeed_ref, after_ref, input_ref, out_ref = refs
    sequences = after_ref.shape[0]
    if homes == 2:
        ours, theirs = mixed
        theirs = jnp.concatenate([theirs[sequences:], theirs[:sequences]], axis=0)
        first = at_ref[3] == 0
        mixed = [jnp.where(first, ours, theirs), jnp.where(first, theirs, ours)]
    mixed = jnp.concatenate(mixed, axis=1)
    residual = jnp.concatenate([ref[...].astype(WIDE) for ref in tokens], axis=0)
    after = (residual + rms_scale(mixed, postmix_ref[...])).astype(HALF)
    after_ref[...] = after[:sequences]
    given = rms_scale(after.astype(WIDE), prefeed_ref[...])
    input_ref[...] = given[:sequences].astype(HALF)
    blocks, _, tall, width = out_ref.shape
    dims = (((0,), (0,)), ((), ()))
    for home, hot in enumerate(hots):
        mine = given[home * sequences : (home + 1) * sequences]
        folded = jnp.concatenate(
            [mine[:, at : at + width] for at in range(0, given.shape[1], width)], axis=0
        ).astype(HALF)
        start = at_ref[3] * (blocks * tall) if homes == 2 else 0
        lanes = hot[:, pl.ds(pl.multiple_of(start, blocks * tall), blocks * tall)]
        rows = lax.dot_general(lanes, folded, dims, preferred_element_type=WIDE)
        out_ref[:, home] = rows.astype(HALF).reshape(blocks, tall, width)


def turned(values, by):
    by = by % values.shape[1]
    return pltpu.roll(values, by, 1) if by else values


def hold_gate_kernel(after_ref, weight_ref, held_ref, done):
    load = pltpu.make_async_copy(weight_ref, held_ref, done)
    load.start()
    load.wait()


def expert_kernel(at_ref, came_ref, gate_ref, up_ref, down_ref, out_ref, held_up, held_down, done, *, split
):
    groups, fold, tall, width = came_ref.shape
    capacity = tall // fold
    spans = [pl.ds(part * width, width) for part in range(fold)]
    loads = [(up_ref.at[span], held_up.at[span]) for span in spans]
    loads += [(down_ref.at[:, span], held_down.at[:, span]) for span in spans]
    loads = [
        pltpu.make_async_copy(source, target, done.at[number])
        for number, (source, target) in enumerate(loads)
    ]
    for load in loads:
        load.start()
    area = lax.broadcasted_iota(jnp.int32, (groups, tall, width), 1) // capacity
    came = [came_ref[:, at].astype(WIDE) for at in range(fold)]
    gates, ups, given = 0.0, 0.0, []
    for part in range(fold):
        for at in range(fold):
            piece = turned(came[at], (at - part) * capacity)
            rows = piece if at == 0 else jnp.where(area == at, piece, rows)
        given.append(rows.reshape(groups * tall, width).astype(HALF))
        gates = gates + jnp.dot(
            given[part], gate_ref[part * width : (part + 1) * width], preferred_element_type=WIDE
        )
    for part in range(fold):
        loads[part].wait()
        ups = ups + jnp.dot(
            given[part], held_up[part * width : (part + 1) * width], preferred_element_type=WIDE
        )
    hidden = (jax.nn.silu(gates) * ups).astype(HALF)
    answers = []
    for part in range(fold):
        loads[fold + part].wait()
        answer = jnp.dot(
            hidden, held_down[:, part * width : (part + 1) * width], preferred_element_type=WIDE
        )
        answers.append(answer.reshape(groups, tall, width))
    for at in range(fold):
        for part in range(fold):
            piece = turned(answers[part], (part - at) * capacity)
            packed = piece if part == 0 else jnp.where(area == part, piece, packed)
        out_ref[at ^ at_ref[3] if split else at] = packed.astype(HALF)


def shared_kernel(input_ref, gate_ref, up_ref, down_ref, out_ref):
    rows = input_ref[...]
    gates = jnp.dot(rows, gate_ref[...], preferred_element_type=WIDE)
    ups = jnp.dot(rows, up_ref[...], preferred_element_type=WIDE)
    hidden = (jax.nn.silu(gates) * ups).astype(HALF)
    out_ref[...] = jnp.dot(hidden, down_ref[...], preferred_element_type=WIDE)


def final_kernel(back_ref, weights_ref, shared_ref, after_ref, gain_ref, out_ref):
    sequences = out_ref.shape[0]
    picked = jnp.dot(weights_ref[...], back_ref[...], preferred_element_type=WIDE)
    step = 2 * sequences
    routed = jnp.concatenate(
        [
            picked[at : at + sequences] + picked[at + sequences : at + step]
            for at in range(0, picked.shape[0], step)
        ],
        axis=1,
    )
    out_ref[...] = (
        after_ref[...].astype(WIDE) + rms_scale(routed + shared_ref[...], gain_ref[...])
    ).astype(HALF)


def on_device(
    tokens,
    premix_gain,
    postmix_gain,
    prefeed_gain,
    postfeed_gain,
    query_weight,
    key_weight,
    value_weight,
    outgate_weight,
    ingate_weight,
    forget_weight,
    ingate_bias,
    forget_bias,
    memory_state,
    normalizer,
    stabilizer,
    output_weight,
    expert_ids,
    route_weights,
    expert_gate,
    expert_up,
    expert_down,
    shared_gate,
    shared_up,
    shared_down,
):
    sequences, model_width = tokens.shape
    devices = lax.axis_size("ep")
    heads, width = memory_state.shape[1], memory_state.shape[3]
    planes = devices // heads
    chips = heads // 2
    groups = planes // 2
    copies = 1 if groups == 2 else groups
    place = lax.axis_index("ep")
    at = jnp.stack(
        [place % 2, place // 2 % chips, place // heads % 2, place // (2 * heads)]
    ).astype(jnp.int32)

    rows = query_weight.shape[0]
    piece_width = model_width // planes
    local_count = expert_gate.shape[0]
    experts_total = local_count * devices
    choose_count = expert_ids.shape[1]
    capacity = min(
        sequences, max(2, 2 * ((sequences * choose_count + experts_total - 1) // experts_total))
    )
    fold = max(1, 8 // capacity)
    tall = fold * capacity
    slot_count = experts_total * tall
    slot_width = model_width // fold

    kept, sent, held_tokens, normed, pieces = local_call(
        functools.partial(start_kernel, planes=planes),
        [
            ((2, *query_weight.shape), HALF, "v"),
            ((2, *query_weight.shape), HALF, "v"),
            ((sequences, model_width), HALF, "v"),
            ((sequences, model_width), HALF, "v"),
            ((devices, sequences, piece_width), HALF, "h"),
        ],
        (at, tokens, premix_gain[None], query_weight, key_weight, value_weight, outgate_weight),
        "shhhhhh",
        scratch=[pltpu.VMEM((1, model_width), WIDE), pltpu.SemaphoreType.DMA((6,))],
    )
    came = swap(sent, CORE)
    rows_in = exchange(pieces)
    dealt = local_call(
        deal_kernel, [((2 * rows, 4 * width), HALF, "v")] * chips, (at, kept, came), "svv"
    )
    blocks = [dealt[0]] + [swap(dealt[turn], CORE * 2 * turn) for turn in range(1, chips)]

    own_out = output_weight.T[None]
    across_out = swap(own_out, heads)
    (pair,) = local_call(
        merge_kernel, [((2, *own_out.shape[1:]), HALF, "v")], (own_out, across_out)
    )
    ours = [pair] + [swap(pair, CORE * 2 * turn) for turn in range(1, chips)]
    theirs = [swap(block, CORE) for block in ours]
    (mix_weight,) = local_call(
        stack_kernel,
        [((2 * piece_width, heads * width), HALF, "v")],
        (at, *ours, *theirs),
        "s" + "v" * 2 * chips,
    )

    small = (
        ingate_weight.T,
        forget_weight.T,
        ingate_bias[None],
        forget_bias[None],
        stabilizer,
        expert_ids,
        route_weights,
    )
    keep_old, write_new, next_stabilizer, hot, pick, *gains, held_normalizer = local_call(
        functools.partial(prepare_kernel, fold=fold, capacity=capacity),
        [
            ((sequences, heads), WIDE, "v"),
            ((sequences, heads), WIDE, "v"),
            ((sequences, heads), WIDE, "h"),
            ((fold * sequences, slot_count), HALF, "v"),
            ((2 * fold * sequences, slot_count), HALF, "v"),
            ((1, model_width), WIDE, "v"),
            ((1, model_width), WIDE, "v"),
            ((1, model_width), WIDE, "v"),
            (normalizer.shape, WIDE, "v"),
        ],
        (normed, postmix_gain[None], prefeed_gain[None], postfeed_gain[None], normalizer, *small),
        "v" + "h" * 11,
        scratch=[
            *(pltpu.VMEM(array.shape, array.dtype) for array in small),
            pltpu.SemaphoreType.DMA((11,)),
        ],
    )

    (partial,) = local_call(
        project_kernel,
        [((devices * sequences, 4 * width), HALF, "h")],
        (at, rows_in.reshape(devices * sequences, piece_width), *blocks),
        "sv" + "v" * chips,
        scratch=[pltpu.VMEM((piece_width, 4 * width), HALF)],
    )
    partial = partial.reshape(devices, sequences, 4 * width)
    parts = exchange(partial)
    early = 3 * sequences // 8
    (early_memory,) = local_call(
        hold_kernel,
        [((early, *memory_state.shape[1:]), WIDE, "v")],
        (partial, memory_state),
        "hh",
        scratch=[pltpu.SemaphoreType.DMA],
    )
    gated, keys, values = local_call(
        read_kernel,
        [
            ((copies, sequences, heads * width), HALF, "v"),
            ((heads, sequences, width), WIDE, "v"),
            ((heads, sequences, width), WIDE, "v"),
        ],
        (parts, keep_old, write_new, held_normalizer, early_memory, memory_state),
        "vvvvvh",
        scratch=[
            pltpu.VMEM((sequences - early, *memory_state.shape[1:]), WIDE),
            pltpu.SemaphoreType.DMA((sequences - early,)),
        ],
    )
    paired = groups == 2 and fold == 2
    if groups == 2:
        gated_rows = [gated[0], swap(gated[0], 2 * heads)]
        (own_mixed,) = local_call(
            mix_kernel,
            [((2 * sequences, 2 * piece_width), HALF, "v")],
            (*gated_rows, mix_weight),
        )
        mixed = [own_mixed, swap(own_mixed, 2 * heads)]
        if not paired:
            theirs = mixed[1][sequences:]
            first = at[3] == 0
            mixed = [
                jnp.where(first, own_mixed[:sequences], theirs),
                jnp.where(first, theirs, own_mixed[:sequences]),
            ]
    else:
        lines = [[low + 2 * heads * at for at in range(groups)] for low in range(2 * heads)]
        gathered = exchange(gated, lines).reshape(groups * sequences, heads * width)
        (mixed,) = local_call(
            mix_kernel,
            [((groups * sequences, 2 * piece_width), HALF, "h")],
            (gathered, mix_weight),
        )
        mixed = exchange(mixed.reshape(groups, sequences, 2 * piece_width), lines)
        mixed = [mixed[number] for number in range(groups)]
    homes = 2 if paired else 1
    held, hots, members = [held_tokens], [hot], None
    if paired:
        held.append(swap(held_tokens, 2 * heads))
        hots.append(swap(hot, 2 * heads))
        half = devices // 2
        members = [list(range(half)), list(range(half, devices))]
    after_mix, expert_input, outgoing = local_call(
        functools.partial(send_kernel, pieces=len(mixed)),
        [
            ((sequences, model_width), HALF, "v"),
            ((sequences, model_width), HALF, "v"),
            ((experts_total // homes, homes, tall, slot_width), HALF, "h"),
        ],
        (at, *mixed, *held, *hots, gains[0], gains[1]),
        "s" + "v" * (len(mixed) + 2 * homes + 2),
    )
    outgoing = outgoing.reshape(experts_total // homes, homes * tall, slot_width)
    arrived = exchange(outgoing, members)
    arrived = arrived.reshape(devices // homes, local_count, homes * tall, slot_width)
    answers = []
    for expert in range(local_count):
        (held_gate,) = local_call(
            hold_gate_kernel,
            [(expert_gate.shape[1:], HALF, "v")],
            (after_mix, expert_gate[expert]),
            "vh",
            scratch=[pltpu.SemaphoreType.DMA],
        )
        (answer,) = local_call(
            functools.partial(expert_kernel, split=paired),
            [((fold, devices // fold, tall, slot_width), HALF, "h")],
            (
                at,
                arrived[:, expert].reshape(devices // fold, fold, tall, slot_width),
                held_gate,
                expert_up[expert],
                expert_down[expert],
            ),
            "svvhh",
            scratch=[
                pltpu.VMEM(expert_up.shape[1:], HALF),
                pltpu.VMEM(expert_down.shape[1:], HALF),
                pltpu.SemaphoreType.DMA((2 * fold,)),
            ],
        )
        if not paired:
            answer = answer.swapaxes(0, 1)
        answers.append(answer.reshape(devices, tall, slot_width))
    answered = jnp.stack(answers, axis=1).reshape(experts_total, tall, slot_width)
    returned = exchange(answered)

    (shared_out,) = local_call(
        shared_kernel,
        [((sequences, model_width), WIDE, "v")],
        (expert_input, shared_gate, shared_up, shared_down),
    )
    key_rows, value_rows = keys.swapaxes(0, 1), values.swapaxes(0, 1)
    next_memory = (
        keep_old[..., None, None] * memory_state
        + write_new[..., None, None] * value_rows[..., :, None] * key_rows[..., None, :]
    )
    next_normalizer = keep_old[..., None] * normalizer + write_new[..., None] * key_rows
    (next_tokens,) = local_call(
        final_kernel,
        [((sequences, model_width), HALF, "h")],
        (returned.reshape(slot_count, slot_width), pick, shared_out, after_mix, gains[2]),
    )
    return (next_tokens, next_memory, next_normalizer, next_stabilizer)


def solution(mesh):
    in_specs = (
        P("ep", None),
        P(),
        P(),
        P(),
        P(),
        P("ep", None),
        P("ep", None),
        P("ep", None),
        P("ep", None),
        P(),
        P(),
        P(),
        P(),
        P("ep", None, None, None),
        P("ep", None, None),
        P("ep", None),
        P(None, "ep"),
        P("ep", None),
        P("ep", None),
        P("ep", None, None),
        P("ep", None, None),
        P("ep", None, None),
        P(),
        P(),
        P(),
    )
    out_specs = (P("ep", None), P("ep", None, None, None), P("ep", None, None), P("ep", None))

    return jax.shard_map(
        on_device, mesh=mesh, in_specs=in_specs, out_specs=out_specs, check_vma=False
    )
```

```python
import functools
import jax
import jax.numpy as jnp
from jax import lax
from jax.experimental import pallas as pl
from jax.experimental.pallas import tpu as pltpu
from jax.sharding import PartitionSpec as P

epsilon = 1e-06
CORE = 1
WIDE, HALF = jnp.float32, jnp.bfloat16


def rms_scale(values, gain_row):
    return (
        values * lax.rsqrt(jnp.mean(values * values, axis=-1, keepdims=True) + epsilon) * gain_row
    )


def swap(values, bit):
    devices = lax.axis_size("ep")
    return lax.ppermute(values, "ep", [(i, i ^ bit) for i in range(devices)])


def exchange(values, groups=None):
    return lax.all_to_all(
        values, "ep", split_axis=0, concat_axis=0, tiled=True, axis_index_groups=groups
    )


SPACES = {"v": pltpu.VMEM, "h": pltpu.HBM, "s": pltpu.SMEM}


def local_call(body, outs, args, spaces=None, scratch=(), limit=16):
    spaces = spaces or "v" * len(args)
    args = [
        pltpu.with_memory_space_constraint(arg, SPACES[space]) if space != "s" else arg
        for arg, space in zip(args, spaces)
    ]
    return pl.pallas_call(
        body,
        out_shape=[SPACES[space](shape, kind) for shape, kind, space in outs],
        in_specs=[pl.BlockSpec(memory_space=SPACES[space]) for space in spaces],
        out_specs=[pl.BlockSpec(memory_space=pltpu.VMEM)] * len(outs),
        scratch_shapes=list(scratch),
        compiler_params=pltpu.CompilerParams(vmem_limit_bytes=limit * 2**20),
    )(*args)


def fetch(pairs, done):
    copies = [
        pltpu.make_async_copy(source, target, done.at[number])
        for number, (source, target) in enumerate(pairs)
    ]
    for copy in copies:
        copy.start()
    for copy in copies:
        copy.wait()


def start_kernel(tokens_ref, gain_ref, *refs, planes):
    core = lax.axis_index("ep") % 2
    weights, outs, (scale_ref, done) = refs[:4], refs[4:-2], refs[-2:]
    kept_ref, sent_ref, held_ref, normed_ref, pieces_ref = outs
    loads = [
        pltpu.make_async_copy(source, target, done.at[number])
        for number, (source, target) in enumerate([(tokens_ref, held_ref), (gain_ref, scale_ref)])
    ]
    for load in loads:
        load.start()

    def place(kept, sent):
        pairs = [(weight, kept_ref.at[number]) for number, weight in enumerate(kept)]
        pairs += [(weight, sent_ref.at[number]) for number, weight in enumerate(sent)]
        for number, (source, target) in enumerate(pairs):
            pltpu.make_async_copy(source, target, done.at[2 + number]).start()

    pl.when(core == 0)(lambda: place(weights[:2], weights[2:]))
    pl.when(core != 0)(lambda: place(weights[2:], weights[:2]))
    for load in loads:
        load.wait()
    normed = rms_scale(held_ref[...].astype(WIDE), scale_ref[...]).astype(HALF)
    normed_ref[...] = normed
    width = normed.shape[1] // planes
    copies = pieces_ref.shape[0] // planes
    for plane in range(planes):
        piece = normed[:, plane * width : (plane + 1) * width]
        for copy in range(copies):
            pieces_ref[plane * copies + copy] = piece
    for number in range(2):
        for side, target in enumerate((kept_ref, sent_ref)):
            source = weights[number]
            pltpu.make_async_copy(source, target.at[number], done.at[2 + 2 * side + number]).wait()


def deal_kernel(at_ref, kept_ref, came_ref, *outs):
    core, chip = at_ref[0], at_ref[1]
    count, rows, _ = kept_ref.shape
    lanes = outs[0].shape[1] // count
    mine = pl.multiple_of(core * rows, rows)
    other = pl.multiple_of((1 - core) * rows, rows)
    for turn, out in enumerate(outs):
        start = pl.multiple_of((chip ^ turn) * lanes, lanes)
        for number in range(count):
            across = slice(number * lanes, (number + 1) * lanes)
            out[pl.ds(mine, rows), across] = kept_ref[number, :, pl.ds(start, lanes)]
            out[pl.ds(other, rows), across] = came_ref[number, :, pl.ds(start, lanes)]


def prepare_kernel(
    normed_ref, *refs, fold, capacity
):
    sources, outs, held, done = refs[:11], refs[11:20], refs[20:-1], refs[-1]
    keep_ref, write_ref, next_ref, hot_ref, pick_ref = outs[:5]
    fetch(list(zip(sources, outs[5:] + held)), done)
    ingate_ref, forget_ref, ingate_bias, forget_bias, stabilizer_ref, ids_ref, route_ref = held
    normed = normed_ref[...]
    dims = (((1,), (1,)), ((), ()))
    input_pre = lax.dot_general(normed, ingate_ref[...], dims, preferred_element_type=WIDE)
    input_pre = input_pre + ingate_bias[...]
    forget_pre = lax.dot_general(normed, forget_ref[...], dims, preferred_element_type=WIDE)
    forget_pre = forget_pre + forget_bias[...]
    carried = jax.nn.log_sigmoid(forget_pre) + stabilizer_ref[...]
    following = jnp.maximum(carried, input_pre)
    next_ref[...] = following
    keep_ref[...] = jnp.exp(carried - following)
    write_ref[...] = jnp.exp(input_pre - following)

    sequences, choose_count = ids_ref.shape
    slots = hot_ref.shape[1]
    slot = lax.broadcasted_iota(jnp.int32, (sequences, slots), 1)
    order = lax.broadcasted_iota(jnp.int32, (sequences, slots), 0)
    expert = slot // (fold * capacity)
    named = jnp.zeros((sequences, slots), WIDE)
    share = jnp.zeros((sequences, slots), WIDE)
    for choice in range(choose_count):
        match = ids_ref[:, choice : choice + 1] == expert
        named = jnp.where(match, 1.0, named)
        share = jnp.where(match, route_ref[:, choice : choice + 1], share)
    rank = jnp.zeros((sequences, slots), WIDE)
    for earlier in range(sequences - 1):
        rank = rank + jnp.where(order > earlier, named[earlier : earlier + 1], 0.0)
    taken = (named > 0.0) & (rank == (slot % capacity).astype(WIDE))
    part_of = (slot // capacity) % fold
    high = share.astype(HALF).astype(WIDE)
    low = share - high
    for part in range(fold):
        here = taken & (part_of == part)
        rows = slice(part * sequences, (part + 1) * sequences)
        hot_ref[rows] = jnp.where(here, 1.0, 0.0).astype(HALF)
        start = 2 * part * sequences
        pick_ref[start : start + sequences] = jnp.where(here, high, 0.0).astype(HALF)
        pick_ref[start + sequences : start + 2 * sequences] = jnp.where(here, low, 0.0).astype(HALF)


def project_kernel(at_ref, rows_ref, *refs):
    blocks, out_ref, held_ref = refs[:-2], refs[-2], refs[-1]
    chip = at_ref[1]
    depth = blocks[0].shape[0]
    for turn, block in enumerate(blocks):
        start = pl.multiple_of((chip ^ turn) * depth, depth)
        held_ref[pl.ds(start, depth), :] = block[...]
    out_ref[...] = jnp.dot(
        rows_ref[...], held_ref[...], preferred_element_type=WIDE
    ).astype(HALF)


def hold_kernel(after_ref, memory_ref, held_ref, done):
    load = pltpu.make_async_copy(memory_ref.at[pl.ds(0, held_ref.shape[0])], held_ref, done)
    load.start()
    load.wait()


def read_kernel(*refs):
    parts_ref, keep_ref, write_ref, normalizer_ref, early_ref, memory_ref = refs[:6]
    side, (gated_ref, keys_ref, values_ref, late_ref, done) = refs[6:-5], refs[-5:]
    early = early_ref.shape[0]
    loads = [
        pltpu.make_async_copy(memory_ref.at[early + at], late_ref.at[at], done.at[at])
        for at in range(late_ref.shape[0])
    ]
    for load in loads:
        load.start()
    start = memory_ref.shape[1] * memory_ref.shape[3]
    for ref in side:
        for row in range(0, ref.shape[0], gated_ref.shape[1]):
            gated_ref[0, :, start : start + ref.shape[1]] = ref[row : row + gated_ref.shape[1]]
            start += ref.shape[1]
    copies, sequences, _ = gated_ref.shape
    heads, width = memory_ref.shape[1], memory_ref.shape[3]
    planes = parts_ref.shape[0] // heads
    row = lax.broadcasted_iota(jnp.int32, (sequences, width), 0)
    pieces, asked = [], []
    for head in range(heads):
        first = head % 2 * width
        found = []
        for core in range(2):
            for start in (first, first + 2 * width):
                total = 0.0
                for plane in range(planes):
                    part = parts_ref[plane * heads + head // 2 * 2 + core]
                    total = total + part[:, start : start + width].astype(WIDE)
                found.append(total)
        found[1] = found[1] * width ** (-0.5)
        keys_ref[head] = found[1]
        values_ref[head] = found[2]
        pieces.append(found)
        high = found[0].astype(HALF)
        low = (found[0] - high.astype(WIDE)).astype(HALF)
        both = jnp.concatenate([high, low], axis=0)
        asked.append(jnp.concatenate([both, both], axis=1))
    dims = (((1,), (1,)), ((), ()))
    reads = [jnp.zeros((sequences, width), WIDE)] * heads
    for sequence in range(sequences):
        if sequence >= early:
            loads[sequence - early].wait()
        for first in range(0, heads, 2):
            held = []
            for head in (first, first + 1):
                if sequence < early:
                    memory = early_ref[sequence, head]
                else:
                    memory = late_ref[sequence - early, head]
                upper = memory.astype(HALF)
                lower = (memory - upper.astype(WIDE)).astype(HALF)
                held.append(jnp.concatenate([upper, lower], axis=1))
            answer = lax.dot_general(
                jnp.concatenate([asked[first], asked[first + 1]], axis=0),
                jnp.concatenate(held, axis=0),
                dims,
                preferred_element_type=WIDE,
            )
            for side in range(2):
                start = 2 * side * sequences
                mine = answer[start : start + 2 * sequences, side * width : (side + 1) * width]
                mine = mine[:sequences] + mine[sequences:]
                head = first + side
                reads[head] = jnp.where(row == sequence, mine, reads[head])
    for head in range(heads):
        queries, keys, values, gate = pieces[head]
        keep = keep_ref[:, head : head + 1]
        score = write_ref[:, head : head + 1] * jnp.sum(queries * keys, axis=-1, keepdims=True)
        below = (
            keep * jnp.sum(normalizer_ref[:, head] * queries, axis=-1, keepdims=True) + score
        )
        answer = (keep * reads[head] + score * values) / jnp.maximum(jnp.abs(below), 1.0)
        gated = (jax.nn.sigmoid(gate) * answer).astype(HALF)
        for copy in range(copies):
            gated_ref[copy, :, head * width : (head + 1) * width] = gated


def merge_kernel(*refs):
    out_ref = refs[-1]
    for number, block in enumerate(refs[:-1]):
        out_ref[number] = block[0]


def stack_kernel(at_ref, *refs):
    blocks, out_ref = refs[:-1], refs[-1]
    core, chip, side = at_ref[0], at_ref[1], at_ref[2]
    chips = len(blocks) // 2
    count, rows, _ = blocks[0].shape
    for turn in range(chips):
        for number in range(count):
            start = ((side ^ number) * chips + (chip ^ turn)) * 2 * rows
            for block, half in ((blocks[turn], core), (blocks[chips + turn], 1 - core)):
                place = pl.ds(pl.multiple_of(start + half * rows, rows), rows)
                out_ref[place, :] = block[number]


def mix_kernel(*refs):
    depth = refs[-2].shape[1]
    rows = jnp.concatenate([ref[:, :depth] for ref in refs[:-2]], axis=0)
    refs[-1][...] = lax.dot_general(
        rows, refs[-2][...], (((1,), (1,)), ((), ())), preferred_element_type=WIDE
    ).astype(HALF)


def send_kernel(at_ref, *refs, pieces):
    mixed, refs = [piece[...].astype(WIDE) for piece in refs[:pieces]], refs[pieces:]
    tokens, hots = [refs[0][...]], [refs[1]]
    side, refs = refs[2:-5], refs[-5:]
    homes = 1 + len(side)
    postmix_ref, prefeed_ref, after_ref, input_ref, out_ref = refs
    sequences, model_width = after_ref.shape
    slots = hots[0].shape[1]
    if homes == 2:
        start = side[0].shape[1] - hots[0].shape[0] // sequences * slots
        tokens.append(side[0][:, start - model_width : start])
        hots.append(side[0].at[:, pl.ds(start, side[0].shape[1] - start)])
        ours, theirs = mixed
        theirs = jnp.concatenate([theirs[sequences:], theirs[:sequences]], axis=0)
        first = at_ref[3] == 0
        mixed = [jnp.where(first, ours, theirs), jnp.where(first, theirs, ours)]
    mixed = jnp.concatenate(mixed, axis=1)
    residual = jnp.concatenate([rows.astype(WIDE) for rows in tokens], axis=0)
    after = (residual + rms_scale(mixed, postmix_ref[...])).astype(HALF)
    after_ref[...] = after[:sequences]
    given = rms_scale(after.astype(WIDE), prefeed_ref[...])
    input_ref[...] = given[:sequences].astype(HALF)
    blocks, _, tall, width = out_ref.shape
    dims = (((0,), (0,)), ((), ()))
    start = at_ref[3] * (blocks * tall) if homes == 2 else 0
    step = out_ref.shape[3]
    folded, lanes = [], []
    for home, hot in enumerate(hots):
        mine = given[home * sequences : (home + 1) * sequences]
        folded.append(
            jnp.concatenate([mine[:, at : at + step] for at in range(0, model_width, step)], axis=0)
        )
        lanes.append(
            jnp.concatenate(
                [
                    hot[:, pl.ds(pl.multiple_of(start + at, blocks * tall), blocks * tall)]
                    for at in range(0, hot.shape[1], slots)
                ],
                axis=0,
            ).astype(WIDE)
        )
    for half in range(homes):
        rows, picks = folded[half], lanes[half]
        if homes == 2:
            rows = jnp.where(first, rows, folded[1 - half])
            picks = jnp.where(first, picks, lanes[1 - half])
        rows = lax.dot_general(
            picks.astype(HALF), rows.astype(HALF), dims, preferred_element_type=WIDE
        )
        out_ref[:, half] = rows.astype(HALF).reshape(blocks, tall, width)


def turned(values, by):
    by = by % values.shape[1]
    return pltpu.roll(values, by, 1) if by else values


def hold_gate_kernel(after_ref, weight_ref, held_ref, done):
    load = pltpu.make_async_copy(weight_ref, held_ref, done)
    load.start()
    load.wait()


def expert_kernel(came_ref, gate_ref, up_ref, down_ref, out_ref, held_up, held_down, done
):
    groups, fold, tall, width = came_ref.shape
    capacity = tall // fold
    spans = [pl.ds(part * width, width) for part in range(fold)]
    loads = [(up_ref.at[span], held_up.at[span]) for span in spans]
    loads += [(down_ref.at[:, span], held_down.at[:, span]) for span in spans]
    loads = [
        pltpu.make_async_copy(source, target, done.at[number])
        for number, (source, target) in enumerate(loads)
    ]
    for load in loads:
        load.start()
    area = lax.broadcasted_iota(jnp.int32, (groups, tall, width), 1) // capacity
    came = [came_ref[:, at].astype(WIDE) for at in range(fold)]
    gates, ups, given = 0.0, 0.0, []
    for part in range(fold):
        for at in range(fold):
            piece = turned(came[at], (at - part) * capacity)
            rows = piece if at == 0 else jnp.where(area == at, piece, rows)
        given.append(rows.reshape(groups * tall, width).astype(HALF))
        gates = gates + jnp.dot(
            given[part], gate_ref[part * width : (part + 1) * width], preferred_element_type=WIDE
        )
    for part in range(fold):
        loads[part].wait()
        ups = ups + jnp.dot(
            given[part], held_up[part * width : (part + 1) * width], preferred_element_type=WIDE
        )
    hidden = (jax.nn.silu(gates) * ups).astype(HALF)
    answers = []
    for part in range(fold):
        loads[fold + part].wait()
        answer = jnp.dot(
            hidden, held_down[:, part * width : (part + 1) * width], preferred_element_type=WIDE
        )
        answers.append(answer.reshape(groups, tall, width))
    for at in range(fold):
        for part in range(fold):
            piece = turned(answers[part], (part - at) * capacity)
            packed = piece if part == 0 else jnp.where(area == part, piece, packed)
        out_ref[at] = packed.astype(HALF)


def shared_kernel(input_ref, gate_ref, up_ref, down_ref, out_ref):
    rows = input_ref[...]
    gates = jnp.dot(rows, gate_ref[...], preferred_element_type=WIDE)
    ups = jnp.dot(rows, up_ref[...], preferred_element_type=WIDE)
    hidden = (jax.nn.silu(gates) * ups).astype(HALF)
    out_ref[...] = jnp.dot(hidden, down_ref[...], preferred_element_type=WIDE)


def final_kernel(back_ref, weights_ref, shared_ref, after_ref, gain_ref, out_ref):
    sequences = out_ref.shape[0]
    picked = jnp.dot(weights_ref[...], back_ref[...], preferred_element_type=WIDE)
    step = 2 * sequences
    routed = jnp.concatenate(
        [
            picked[at : at + sequences] + picked[at + sequences : at + step]
            for at in range(0, picked.shape[0], step)
        ],
        axis=1,
    )
    out_ref[...] = (
        after_ref[...].astype(WIDE) + rms_scale(routed + shared_ref[...], gain_ref[...])
    ).astype(HALF)


def on_device(
    tokens,
    premix_gain,
    postmix_gain,
    prefeed_gain,
    postfeed_gain,
    query_weight,
    key_weight,
    value_weight,
    outgate_weight,
    ingate_weight,
    forget_weight,
    ingate_bias,
    forget_bias,
    memory_state,
    normalizer,
    stabilizer,
    output_weight,
    expert_ids,
    route_weights,
    expert_gate,
    expert_up,
    expert_down,
    shared_gate,
    shared_up,
    shared_down,
):
    sequences, model_width = tokens.shape
    devices = lax.axis_size("ep")
    heads, width = memory_state.shape[1], memory_state.shape[3]
    planes = devices // heads
    chips = heads // 2
    groups = planes // 2
    copies = 1 if groups == 2 else groups
    place = lax.axis_index("ep")
    at = jnp.stack(
        [place % 2, place // 2 % chips, place // heads % 2, place // (2 * heads)]
    ).astype(jnp.int32)

    rows = query_weight.shape[0]
    piece_width = model_width // planes
    local_count = expert_gate.shape[0]
    experts_total = local_count * devices
    choose_count = expert_ids.shape[1]
    capacity = min(
        sequences, max(2, 2 * ((sequences * choose_count + experts_total - 1) // experts_total))
    )
    fold = max(1, 8 // capacity)
    tall = fold * capacity
    slot_count = experts_total * tall
    slot_width = model_width // fold

    kept, sent, held_tokens, normed, pieces = local_call(
        functools.partial(start_kernel, planes=planes),
        [
            ((2, *query_weight.shape), HALF, "v"),
            ((2, *query_weight.shape), HALF, "v"),
            ((sequences, model_width), HALF, "v"),
            ((sequences, model_width), HALF, "v"),
            ((devices, sequences, piece_width), HALF, "h"),
        ],
        (tokens, premix_gain[None], query_weight, key_weight, value_weight, outgate_weight),
        "hhhhhh",
        scratch=[pltpu.VMEM((1, model_width), WIDE), pltpu.SemaphoreType.DMA((6,))],
    )
    came = swap(sent, CORE)
    rows_in = exchange(pieces)
    dealt = local_call(
        deal_kernel, [((2 * rows, 4 * width), HALF, "v")] * chips, (at, kept, came), "svv"
    )
    blocks = [dealt[0]] + [swap(dealt[turn], CORE * 2 * turn) for turn in range(1, chips)]

    own_out = output_weight.T[None]
    across_out = swap(own_out, heads)
    (pair,) = local_call(
        merge_kernel, [((2, *own_out.shape[1:]), HALF, "v")], (own_out, across_out)
    )
    ours = [pair] + [swap(pair, CORE * 2 * turn) for turn in range(1, chips)]
    theirs = [swap(block, CORE) for block in ours]
    (mix_weight,) = local_call(
        stack_kernel,
        [((2 * piece_width, heads * width), HALF, "v")],
        (at, *ours, *theirs),
        "s" + "v" * 2 * chips,
    )

    small = (
        ingate_weight.T,
        forget_weight.T,
        ingate_bias[None],
        forget_bias[None],
        stabilizer,
        expert_ids,
        route_weights,
    )
    keep_old, write_new, next_stabilizer, hot, pick, *gains, held_normalizer = local_call(
        functools.partial(prepare_kernel, fold=fold, capacity=capacity),
        [
            ((sequences, heads), WIDE, "v"),
            ((sequences, heads), WIDE, "v"),
            ((sequences, heads), WIDE, "h"),
            ((fold * sequences, slot_count), HALF, "v"),
            ((2 * fold * sequences, slot_count), HALF, "v"),
            ((1, model_width), WIDE, "v"),
            ((1, model_width), WIDE, "v"),
            ((1, model_width), WIDE, "v"),
            (normalizer.shape, WIDE, "v"),
        ],
        (normed, postmix_gain[None], prefeed_gain[None], postfeed_gain[None], normalizer, *small),
        "v" + "h" * 11,
        scratch=[
            *(pltpu.VMEM(array.shape, array.dtype) for array in small),
            pltpu.SemaphoreType.DMA((11,)),
        ],
    )

    (partial,) = local_call(
        project_kernel,
        [((devices * sequences, 4 * width), HALF, "h")],
        (at, rows_in.reshape(devices * sequences, piece_width), *blocks),
        "sv" + "v" * chips,
        scratch=[pltpu.VMEM((piece_width, 4 * width), HALF)],
    )
    partial = partial.reshape(devices, sequences, 4 * width)
    parts = exchange(partial)
    early = 3 * sequences // 8
    (early_memory,) = local_call(
        hold_kernel,
        [((early, *memory_state.shape[1:]), WIDE, "v")],
        (partial, memory_state),
        "hh",
        scratch=[pltpu.SemaphoreType.DMA],
    )
    paired = groups == 2 and fold == 2
    side = (held_tokens, hot) if paired else ()
    payload = heads * width + (model_width + fold * slot_count if paired else 0)
    gated, keys, values = local_call(
        read_kernel,
        [
            ((copies, sequences, payload), HALF, "v"),
            ((heads, sequences, width), WIDE, "v"),
            ((heads, sequences, width), WIDE, "v"),
        ],
        (parts, keep_old, write_new, held_normalizer, early_memory, memory_state, *side),
        "vvvvvh" + "v" * len(side),
        scratch=[
            pltpu.VMEM((sequences - early, *memory_state.shape[1:]), WIDE),
            pltpu.SemaphoreType.DMA((sequences - early,)),
        ],
    )
    if groups == 2:
        gated_rows = [gated[0], swap(gated[0], 2 * heads)]
        (own_mixed,) = local_call(
            mix_kernel,
            [((2 * sequences, 2 * piece_width), HALF, "v")],
            (*gated_rows, mix_weight),
        )
        mixed = [own_mixed, swap(own_mixed, 2 * heads)]
        if not paired:
            theirs = mixed[1][sequences:]
            first = at[3] == 0
            mixed = [
                jnp.where(first, own_mixed[:sequences], theirs),
                jnp.where(first, theirs, own_mixed[:sequences]),
            ]
    else:
        lines = [[low + 2 * heads * at for at in range(groups)] for low in range(2 * heads)]
        gathered = exchange(gated, lines).reshape(groups * sequences, heads * width)
        (mixed,) = local_call(
            mix_kernel,
            [((groups * sequences, 2 * piece_width), HALF, "h")],
            (gathered, mix_weight),
        )
        mixed = exchange(mixed.reshape(groups, sequences, 2 * piece_width), lines)
        mixed = [mixed[number] for number in range(groups)]
    homes = 2 if paired else 1
    members = None
    if paired:
        half = devices // 2
        members = [list(range(half)), list(range(half, devices))]
    side = gated_rows[1:] if paired else []
    after_mix, expert_input, outgoing = local_call(
        functools.partial(send_kernel, pieces=len(mixed)),
        [
            ((sequences, model_width), HALF, "v"),
            ((sequences, model_width), HALF, "v"),
            ((experts_total // homes, homes, tall, slot_width), HALF, "h"),
        ],
        (at, *mixed, held_tokens, hot, *side, gains[0], gains[1]),
        "s" + "v" * (len(mixed) + len(side) + 4),
    )
    outgoing = outgoing.reshape(experts_total // homes, homes * tall, slot_width)
    arrived = exchange(outgoing, members)
    arrived = arrived.reshape(devices // homes, local_count, homes * tall, slot_width)
    answers = []
    for expert in range(local_count):
        (held_gate,) = local_call(
            hold_gate_kernel,
            [(expert_gate.shape[1:], HALF, "v")],
            (after_mix, expert_gate[expert]),
            "vh",
            scratch=[pltpu.SemaphoreType.DMA],
        )
        (answer,) = local_call(
            expert_kernel,
            [((fold, devices // fold, tall, slot_width), HALF, "h")],
            (
                arrived[:, expert].reshape(devices // fold, fold, tall, slot_width),
                held_gate,
                expert_up[expert],
                expert_down[expert],
            ),
            "vvhh",
            scratch=[
                pltpu.VMEM(expert_up.shape[1:], HALF),
                pltpu.VMEM(expert_down.shape[1:], HALF),
                pltpu.SemaphoreType.DMA((2 * fold,)),
            ],
        )
        if not paired:
            answer = answer.swapaxes(0, 1)
        answers.append(answer.reshape(devices, tall, slot_width))
    answered = jnp.stack(answers, axis=1).reshape(experts_total, tall, slot_width)
    returned = exchange(answered)

    (shared_out,) = local_call(
        shared_kernel,
        [((sequences, model_width), WIDE, "v")],
        (expert_input, shared_gate, shared_up, shared_down),
    )
    key_rows, value_rows = keys.swapaxes(0, 1), values.swapaxes(0, 1)
    next_memory = (
        keep_old[..., None, None] * memory_state
        + write_new[..., None, None] * value_rows[..., :, None] * key_rows[..., None, :]
    )
    next_normalizer = keep_old[..., None] * normalizer + write_new[..., None] * key_rows
    (next_tokens,) = local_call(
        final_kernel,
        [((sequences, model_width), HALF, "h")],
        (returned.reshape(slot_count, slot_width), pick, shared_out, after_mix, gains[2]),
    )
    return (next_tokens, next_memory, next_normalizer, next_stabilizer)


def solution(mesh):
    in_specs = (
        P("ep", None),
        P(),
        P(),
        P(),
        P(),
        P("ep", None),
        P("ep", None),
        P("ep", None),
        P("ep", None),
        P(),
        P(),
        P(),
        P(),
        P("ep", None, None, None),
        P("ep", None, None),
        P("ep", None),
        P(None, "ep"),
        P("ep", None),
        P("ep", None),
        P("ep", None, None),
        P("ep", None, None),
        P("ep", None, None),
        P(),
        P(),
        P(),
    )
    out_specs = (P("ep", None), P("ep", None, None, None), P("ep", None, None), P("ep", None))

    return jax.shard_map(
        on_device, mesh=mesh, in_specs=in_specs, out_specs=out_specs, check_vma=False
    )
```

```python
import functools
import jax
import jax.numpy as jnp
from jax import lax
from jax.experimental import pallas as pl
from jax.experimental.pallas import tpu as pltpu
from jax.sharding import PartitionSpec as P

epsilon = 1e-06
CORE = 1
WIDE, HALF = jnp.float32, jnp.bfloat16


def rms_scale(values, gain_row):
    return (
        values * lax.rsqrt(jnp.mean(values * values, axis=-1, keepdims=True) + epsilon) * gain_row
    )


def swap(values, bit):
    devices = lax.axis_size("ep")
    return lax.ppermute(values, "ep", [(i, i ^ bit) for i in range(devices)])


def exchange(values, groups=None):
    return lax.all_to_all(
        values, "ep", split_axis=0, concat_axis=0, tiled=True, axis_index_groups=groups
    )


SPACES = {"v": pltpu.VMEM, "h": pltpu.HBM, "s": pltpu.SMEM}


def local_call(body, outs, args, spaces=None, scratch=(), limit=16):
    spaces = spaces or "v" * len(args)
    args = [
        pltpu.with_memory_space_constraint(arg, SPACES[space]) if space != "s" else arg
        for arg, space in zip(args, spaces)
    ]
    return pl.pallas_call(
        body,
        out_shape=[SPACES[space](shape, kind) for shape, kind, space in outs],
        in_specs=[pl.BlockSpec(memory_space=SPACES[space]) for space in spaces],
        out_specs=[pl.BlockSpec(memory_space=pltpu.VMEM)] * len(outs),
        scratch_shapes=list(scratch),
        compiler_params=pltpu.CompilerParams(vmem_limit_bytes=limit * 2**20),
    )(*args)


def fetch(pairs, done):
    copies = [
        pltpu.make_async_copy(source, target, done.at[number])
        for number, (source, target) in enumerate(pairs)
    ]
    for copy in copies:
        copy.start()
    for copy in copies:
        copy.wait()


def start_kernel(tokens_ref, gain_ref, *refs, planes):
    core = lax.axis_index("ep") % 2
    weights, outs, (scale_ref, done) = refs[:4], refs[4:-2], refs[-2:]
    kept_ref, sent_ref, held_ref, normed_ref, pieces_ref = outs
    loads = [
        pltpu.make_async_copy(source, target, done.at[number])
        for number, (source, target) in enumerate([(tokens_ref, held_ref), (gain_ref, scale_ref)])
    ]
    for load in loads:
        load.start()

    def place(kept, sent):
        pairs = [(weight, kept_ref.at[number]) for number, weight in enumerate(kept)]
        pairs += [(weight, sent_ref.at[number]) for number, weight in enumerate(sent)]
        for number, (source, target) in enumerate(pairs):
            pltpu.make_async_copy(source, target, done.at[2 + number]).start()

    pl.when(core == 0)(lambda: place(weights[:2], weights[2:]))
    pl.when(core != 0)(lambda: place(weights[2:], weights[:2]))
    for load in loads:
        load.wait()
    normed = rms_scale(held_ref[...].astype(WIDE), scale_ref[...]).astype(HALF)
    normed_ref[...] = normed
    width = normed.shape[1] // planes
    copies = pieces_ref.shape[0] // planes
    for plane in range(planes):
        piece = normed[:, plane * width : (plane + 1) * width]
        for copy in range(copies):
            pieces_ref[plane * copies + copy] = piece
    for number in range(2):
        for side, target in enumerate((kept_ref, sent_ref)):
            source = weights[number]
            pltpu.make_async_copy(source, target.at[number], done.at[2 + 2 * side + number]).wait()


def deal_kernel(at_ref, kept_ref, came_ref, *outs):
    core, chip = at_ref[0], at_ref[1]
    count, rows, _ = kept_ref.shape
    lanes = outs[0].shape[1] // count
    mine = pl.multiple_of(core * rows, rows)
    other = pl.multiple_of((1 - core) * rows, rows)
    for turn, out in enumerate(outs):
        start = pl.multiple_of((chip ^ turn) * lanes, lanes)
        for number in range(count):
            across = slice(number * lanes, (number + 1) * lanes)
            out[pl.ds(mine, rows), across] = kept_ref[number, :, pl.ds(start, lanes)]
            out[pl.ds(other, rows), across] = came_ref[number, :, pl.ds(start, lanes)]


def prepare_kernel(
    normed_ref, *refs, fold, capacity
):
    sources, outs, held, done = refs[:11], refs[11:20], refs[20:-1], refs[-1]
    keep_ref, write_ref, next_ref, hot_ref, pick_ref = outs[:5]
    fetch(list(zip(sources, outs[5:] + held)), done)
    ingate_ref, forget_ref, ingate_bias, forget_bias, stabilizer_ref, ids_ref, route_ref = held
    normed = normed_ref[...]
    dims = (((1,), (1,)), ((), ()))
    input_pre = lax.dot_general(normed, ingate_ref[...], dims, preferred_element_type=WIDE)
    input_pre = input_pre + ingate_bias[...]
    forget_pre = lax.dot_general(normed, forget_ref[...], dims, preferred_element_type=WIDE)
    forget_pre = forget_pre + forget_bias[...]
    carried = jax.nn.log_sigmoid(forget_pre) + stabilizer_ref[...]
    following = jnp.maximum(carried, input_pre)
    next_ref[...] = following
    keep_ref[...] = jnp.exp(carried - following)
    write_ref[...] = jnp.exp(input_pre - following)

    sequences, choose_count = ids_ref.shape
    slots = hot_ref.shape[1]
    slot = lax.broadcasted_iota(jnp.int32, (sequences, slots), 1)
    order = lax.broadcasted_iota(jnp.int32, (sequences, slots), 0)
    expert = slot // (fold * capacity)
    named = jnp.zeros((sequences, slots), WIDE)
    share = jnp.zeros((sequences, slots), WIDE)
    for choice in range(choose_count):
        match = ids_ref[:, choice : choice + 1] == expert
        named = jnp.where(match, 1.0, named)
        share = jnp.where(match, route_ref[:, choice : choice + 1], share)
    rank = jnp.zeros((sequences, slots), WIDE)
    for earlier in range(sequences - 1):
        rank = rank + jnp.where(order > earlier, named[earlier : earlier + 1], 0.0)
    taken = (named > 0.0) & (rank == (slot % capacity).astype(WIDE))
    part_of = (slot // capacity) % fold
    high = share.astype(HALF).astype(WIDE)
    low = share - high
    for part in range(fold):
        here = taken & (part_of == part)
        rows = slice(part * sequences, (part + 1) * sequences)
        hot_ref[rows] = jnp.where(here, 1.0, 0.0).astype(HALF)
        start = 2 * part * sequences
        pick_ref[start : start + sequences] = jnp.where(here, high, 0.0).astype(HALF)
        pick_ref[start + sequences : start + 2 * sequences] = jnp.where(here, low, 0.0).astype(HALF)


def project_kernel(at_ref, rows_ref, *refs):
    blocks, out_ref, held_ref = refs[:-2], refs[-2], refs[-1]
    chip = at_ref[1]
    depth = blocks[0].shape[0]
    for turn, block in enumerate(blocks):
        start = pl.multiple_of((chip ^ turn) * depth, depth)
        held_ref[pl.ds(start, depth), :] = block[...]
    out_ref[...] = jnp.dot(
        rows_ref[...], held_ref[...], preferred_element_type=WIDE
    ).astype(HALF)


def hold_kernel(after_ref, memory_ref, held_ref, done):
    load = pltpu.make_async_copy(memory_ref.at[pl.ds(0, held_ref.shape[0])], held_ref, done)
    load.start()
    load.wait()


def read_kernel(*refs):
    parts_ref, keep_ref, write_ref, normalizer_ref, early_ref, memory_ref = refs[:6]
    side, (gated_ref, keys_ref, values_ref, late_ref, done) = refs[6:-5], refs[-5:]
    early = early_ref.shape[0]
    loads = [
        pltpu.make_async_copy(memory_ref.at[early + at], late_ref.at[at], done.at[at])
        for at in range(late_ref.shape[0])
    ]
    for load in loads:
        load.start()
    start = memory_ref.shape[1] * memory_ref.shape[3]
    for ref in side:
        for row in range(0, ref.shape[0], gated_ref.shape[1]):
            gated_ref[0, :, start : start + ref.shape[1]] = ref[row : row + gated_ref.shape[1]]
            start += ref.shape[1]
    copies, sequences, _ = gated_ref.shape
    heads, width = memory_ref.shape[1], memory_ref.shape[3]
    planes = parts_ref.shape[0] // heads
    row = lax.broadcasted_iota(jnp.int32, (sequences, width), 0)
    pieces, asked = [], []
    for head in range(heads):
        first = head % 2 * width
        found = []
        for core in range(2):
            for start in (first, first + 2 * width):
                total = 0.0
                for plane in range(planes):
                    part = parts_ref[plane * heads + head // 2 * 2 + core]
                    total = total + part[:, start : start + width].astype(WIDE)
                found.append(total)
        found[1] = found[1] * width ** (-0.5)
        keys_ref[head] = found[1]
        values_ref[head] = found[2]
        pieces.append(found)
        high = found[0].astype(HALF)
        low = (found[0] - high.astype(WIDE)).astype(HALF)
        both = jnp.concatenate([high, low], axis=0)
        asked.append(jnp.concatenate([both, both], axis=1))
    dims = (((1,), (1,)), ((), ()))
    reads = [jnp.zeros((sequences, width), WIDE)] * heads
    for sequence in range(sequences):
        if sequence >= early:
            loads[sequence - early].wait()
        for first in range(0, heads, 2):
            held = []
            for head in (first, first + 1):
                if sequence < early:
                    memory = early_ref[sequence, head]
                else:
                    memory = late_ref[sequence - early, head]
                upper = memory.astype(HALF)
                lower = (memory - upper.astype(WIDE)).astype(HALF)
                held.append(jnp.concatenate([upper, lower], axis=1))
            answer = lax.dot_general(
                jnp.concatenate([asked[first], asked[first + 1]], axis=0),
                jnp.concatenate(held, axis=0),
                dims,
                preferred_element_type=WIDE,
            )
            for side in range(2):
                start = 2 * side * sequences
                mine = answer[start : start + 2 * sequences, side * width : (side + 1) * width]
                mine = mine[:sequences] + mine[sequences:]
                head = first + side
                reads[head] = jnp.where(row == sequence, mine, reads[head])
    for head in range(heads):
        queries, keys, values, gate = pieces[head]
        keep = keep_ref[:, head : head + 1]
        score = write_ref[:, head : head + 1] * jnp.sum(queries * keys, axis=-1, keepdims=True)
        below = (
            keep * jnp.sum(normalizer_ref[:, head] * queries, axis=-1, keepdims=True) + score
        )
        answer = (keep * reads[head] + score * values) / jnp.maximum(jnp.abs(below), 1.0)
        gated = (jax.nn.sigmoid(gate) * answer).astype(HALF)
        for copy in range(copies):
            gated_ref[copy, :, head * width : (head + 1) * width] = gated


def merge_kernel(*refs):
    out_ref = refs[-1]
    for number, block in enumerate(refs[:-1]):
        out_ref[number] = block[0]


def stack_kernel(at_ref, *refs):
    blocks, out_ref = refs[:-1], refs[-1]
    core, chip, side = at_ref[0], at_ref[1], at_ref[2]
    chips = len(blocks) // 2
    count, rows, _ = blocks[0].shape
    for turn in range(chips):
        for number in range(count):
            start = ((side ^ number) * chips + (chip ^ turn)) * 2 * rows
            for block, half in ((blocks[turn], core), (blocks[chips + turn], 1 - core)):
                place = pl.ds(pl.multiple_of(start + half * rows, rows), rows)
                out_ref[place, :] = block[number]


def mix_kernel(at_ref, *refs, blocks):
    out_ref, held_ref = refs[-2:]
    stack_kernel(at_ref, *refs[:blocks], held_ref)
    depth = held_ref.shape[1]
    rows = jnp.concatenate([ref[:, :depth] for ref in refs[blocks:-2]], axis=0)
    out_ref[...] = lax.dot_general(
        rows, held_ref[...], (((1,), (1,)), ((), ())), preferred_element_type=WIDE
    ).astype(HALF)


def send_kernel(at_ref, *refs, pieces):
    mixed, refs = [piece[...].astype(WIDE) for piece in refs[:pieces]], refs[pieces:]
    tokens, hots = [refs[0][...]], [refs[1]]
    side, refs = refs[2:-5], refs[-5:]
    homes = 1 + len(side)
    postmix_ref, prefeed_ref, after_ref, input_ref, out_ref = refs
    sequences, model_width = after_ref.shape
    slots = hots[0].shape[1]
    if homes == 2:
        start = side[0].shape[1] - hots[0].shape[0] // sequences * slots
        tokens.append(side[0][:, start - model_width : start])
        hots.append(side[0].at[:, pl.ds(start, side[0].shape[1] - start)])
        ours, theirs = mixed
        theirs = jnp.concatenate([theirs[sequences:], theirs[:sequences]], axis=0)
        first = at_ref[3] == 0
        mixed = [jnp.where(first, ours, theirs), jnp.where(first, theirs, ours)]
    mixed = jnp.concatenate(mixed, axis=1)
    residual = jnp.concatenate([rows.astype(WIDE) for rows in tokens], axis=0)
    after = (residual + rms_scale(mixed, postmix_ref[...])).astype(HALF)
    after_ref[...] = after[:sequences]
    given = rms_scale(after.astype(WIDE), prefeed_ref[...])
    input_ref[...] = given[:sequences].astype(HALF)
    blocks, _, tall, width = out_ref.shape
    dims = (((0,), (0,)), ((), ()))
    start = at_ref[3] * (blocks * tall) if homes == 2 else 0
    step = out_ref.shape[3]
    folded, lanes = [], []
    for home, hot in enumerate(hots):
        mine = given[home * sequences : (home + 1) * sequences]
        folded.append(
            jnp.concatenate([mine[:, at : at + step] for at in range(0, model_width, step)], axis=0)
        )
        lanes.append(
            jnp.concatenate(
                [
                    hot[:, pl.ds(pl.multiple_of(start + at, blocks * tall), blocks * tall)]
                    for at in range(0, hot.shape[1], slots)
                ],
                axis=0,
            ).astype(WIDE)
        )
    for half in range(homes):
        rows, picks = folded[half], lanes[half]
        if homes == 2:
            rows = jnp.where(first, rows, folded[1 - half])
            picks = jnp.where(first, picks, lanes[1 - half])
        rows = lax.dot_general(
            picks.astype(HALF), rows.astype(HALF), dims, preferred_element_type=WIDE
        )
        out_ref[:, half] = rows.astype(HALF).reshape(blocks, tall, width)


def turned(values, by):
    by = by % values.shape[1]
    return pltpu.roll(values, by, 1) if by else values


def hold_gate_kernel(after_ref, weight_ref, held_ref, done):
    load = pltpu.make_async_copy(weight_ref, held_ref, done)
    load.start()
    load.wait()


def expert_kernel(came_ref, gate_ref, up_ref, down_ref, out_ref, held_up, held_down, done
):
    groups, fold, tall, width = came_ref.shape
    capacity = tall // fold
    spans = [pl.ds(part * width, width) for part in range(fold)]
    loads = [(up_ref.at[span], held_up.at[span]) for span in spans]
    loads += [(down_ref.at[:, span], held_down.at[:, span]) for span in spans]
    loads = [
        pltpu.make_async_copy(source, target, done.at[number])
        for number, (source, target) in enumerate(loads)
    ]
    for load in loads:
        load.start()
    area = lax.broadcasted_iota(jnp.int32, (groups, tall, width), 1) // capacity
    came = [came_ref[:, at].astype(WIDE) for at in range(fold)]
    gates, ups, given = 0.0, 0.0, []
    for part in range(fold):
        for at in range(fold):
            piece = turned(came[at], (at - part) * capacity)
            rows = piece if at == 0 else jnp.where(area == at, piece, rows)
        given.append(rows.reshape(groups * tall, width).astype(HALF))
        gates = gates + jnp.dot(
            given[part], gate_ref[part * width : (part + 1) * width], preferred_element_type=WIDE
        )
    for part in range(fold):
        loads[part].wait()
        ups = ups + jnp.dot(
            given[part], held_up[part * width : (part + 1) * width], preferred_element_type=WIDE
        )
    hidden = (jax.nn.silu(gates) * ups).astype(HALF)
    answers = []
    for part in range(fold):
        loads[fold + part].wait()
        answer = jnp.dot(
            hidden, held_down[:, part * width : (part + 1) * width], preferred_element_type=WIDE
        )
        answers.append(answer.reshape(groups, tall, width))
    for at in range(fold):
        for part in range(fold):
            piece = turned(answers[part], (part - at) * capacity)
            packed = piece if part == 0 else jnp.where(area == part, piece, packed)
        out_ref[at] = packed.astype(HALF)


def shared_kernel(input_ref, gate_ref, up_ref, down_ref, out_ref):
    rows = input_ref[...]
    gates = jnp.dot(rows, gate_ref[...], preferred_element_type=WIDE)
    ups = jnp.dot(rows, up_ref[...], preferred_element_type=WIDE)
    hidden = (jax.nn.silu(gates) * ups).astype(HALF)
    out_ref[...] = jnp.dot(hidden, down_ref[...], preferred_element_type=WIDE)


def final_kernel(back_ref, weights_ref, shared_ref, after_ref, gain_ref, out_ref):
    sequences = out_ref.shape[0]
    picked = jnp.dot(weights_ref[...], back_ref[...], preferred_element_type=WIDE)
    step = 2 * sequences
    routed = jnp.concatenate(
        [
            picked[at : at + sequences] + picked[at + sequences : at + step]
            for at in range(0, picked.shape[0], step)
        ],
        axis=1,
    )
    out_ref[...] = (
        after_ref[...].astype(WIDE) + rms_scale(routed + shared_ref[...], gain_ref[...])
    ).astype(HALF)


def on_device(
    tokens,
    premix_gain,
    postmix_gain,
    prefeed_gain,
    postfeed_gain,
    query_weight,
    key_weight,
    value_weight,
    outgate_weight,
    ingate_weight,
    forget_weight,
    ingate_bias,
    forget_bias,
    memory_state,
    normalizer,
    stabilizer,
    output_weight,
    expert_ids,
    route_weights,
    expert_gate,
    expert_up,
    expert_down,
    shared_gate,
    shared_up,
    shared_down,
):
    sequences, model_width = tokens.shape
    devices = lax.axis_size("ep")
    heads, width = memory_state.shape[1], memory_state.shape[3]
    planes = devices // heads
    chips = heads // 2
    groups = planes // 2
    copies = 1 if groups == 2 else groups
    place = lax.axis_index("ep")
    at = jnp.stack(
        [place % 2, place // 2 % chips, place // heads % 2, place // (2 * heads)]
    ).astype(jnp.int32)

    rows = query_weight.shape[0]
    piece_width = model_width // planes
    local_count = expert_gate.shape[0]
    experts_total = local_count * devices
    choose_count = expert_ids.shape[1]
    capacity = min(
        sequences, max(2, 2 * ((sequences * choose_count + experts_total - 1) // experts_total))
    )
    fold = max(1, 8 // capacity)
    tall = fold * capacity
    slot_count = experts_total * tall
    slot_width = model_width // fold

    kept, sent, held_tokens, normed, pieces = local_call(
        functools.partial(start_kernel, planes=planes),
        [
            ((2, *query_weight.shape), HALF, "v"),
            ((2, *query_weight.shape), HALF, "v"),
            ((sequences, model_width), HALF, "v"),
            ((sequences, model_width), HALF, "v"),
            ((devices, sequences, piece_width), HALF, "h"),
        ],
        (tokens, premix_gain[None], query_weight, key_weight, value_weight, outgate_weight),
        "hhhhhh",
        scratch=[pltpu.VMEM((1, model_width), WIDE), pltpu.SemaphoreType.DMA((6,))],
    )
    came = swap(sent, CORE)
    rows_in = exchange(pieces)
    dealt = local_call(
        deal_kernel, [((2 * rows, 4 * width), HALF, "v")] * chips, (at, kept, came), "svv"
    )
    blocks = [dealt[0]] + [swap(dealt[turn], CORE * 2 * turn) for turn in range(1, chips)]

    own_out = output_weight.T[None]
    across_out = swap(own_out, heads)
    (pair,) = local_call(
        merge_kernel, [((2, *own_out.shape[1:]), HALF, "v")], (own_out, across_out)
    )
    ours = [pair] + [swap(pair, CORE * 2 * turn) for turn in range(1, chips)]
    theirs = [swap(block, CORE) for block in ours]
    out_blocks = (*ours, *theirs)
    mix = functools.partial(mix_kernel, blocks=len(out_blocks))
    mix_scratch = [pltpu.VMEM((2 * piece_width, heads * width), HALF)]

    small = (
        ingate_weight.T,
        forget_weight.T,
        ingate_bias[None],
        forget_bias[None],
        stabilizer,
        expert_ids,
        route_weights,
    )
    keep_old, write_new, next_stabilizer, hot, pick, *gains, held_normalizer = local_call(
        functools.partial(prepare_kernel, fold=fold, capacity=capacity),
        [
            ((sequences, heads), WIDE, "v"),
            ((sequences, heads), WIDE, "v"),
            ((sequences, heads), WIDE, "h"),
            ((fold * sequences, slot_count), HALF, "v"),
            ((2 * fold * sequences, slot_count), HALF, "v"),
            ((1, model_width), WIDE, "v"),
            ((1, model_width), WIDE, "v"),
            ((1, model_width), WIDE, "v"),
            (normalizer.shape, WIDE, "v"),
        ],
        (normed, postmix_gain[None], prefeed_gain[None], postfeed_gain[None], normalizer, *small),
        "v" + "h" * 11,
        scratch=[
            *(pltpu.VMEM(array.shape, array.dtype) for array in small),
            pltpu.SemaphoreType.DMA((11,)),
        ],
    )

    (partial,) = local_call(
        project_kernel,
        [((devices * sequences, 4 * width), HALF, "h")],
        (at, rows_in.reshape(devices * sequences, piece_width), *blocks),
        "sv" + "v" * chips,
        scratch=[pltpu.VMEM((piece_width, 4 * width), HALF)],
    )
    partial = partial.reshape(devices, sequences, 4 * width)
    parts = exchange(partial)
    early = 3 * sequences // 8
    (early_memory,) = local_call(
        hold_kernel,
        [((early, *memory_state.shape[1:]), WIDE, "v")],
        (partial, memory_state),
        "hh",
        scratch=[pltpu.SemaphoreType.DMA],
    )
    paired = groups == 2 and fold == 2
    side = (held_tokens, hot) if paired else ()
    payload = heads * width + (model_width + fold * slot_count if paired else 0)
    gated, keys, values = local_call(
        read_kernel,
        [
            ((copies, sequences, payload), HALF, "v"),
            ((heads, sequences, width), WIDE, "v"),
            ((heads, sequences, width), WIDE, "v"),
        ],
        (parts, keep_old, write_new, held_normalizer, early_memory, memory_state, *side),
        "vvvvvh" + "v" * len(side),
        scratch=[
            pltpu.VMEM((sequences - early, *memory_state.shape[1:]), WIDE),
            pltpu.SemaphoreType.DMA((sequences - early,)),
        ],
    )
    if groups == 2:
        gated_rows = [gated[0], swap(gated[0], 2 * heads)]
        (own_mixed,) = local_call(
            mix,
            [((2 * sequences, 2 * piece_width), HALF, "v")],
            (at, *out_blocks, *gated_rows),
            "s" + "v" * (len(out_blocks) + 2),
            mix_scratch,
        )
        mixed = [own_mixed, swap(own_mixed, 2 * heads)]
        if not paired:
            theirs = mixed[1][sequences:]
            first = at[3] == 0
            mixed = [
                jnp.where(first, own_mixed[:sequences], theirs),
                jnp.where(first, theirs, own_mixed[:sequences]),
            ]
    else:
        lines = [[low + 2 * heads * at for at in range(groups)] for low in range(2 * heads)]
        gathered = exchange(gated, lines).reshape(groups * sequences, heads * width)
        (mixed,) = local_call(
            mix,
            [((groups * sequences, 2 * piece_width), HALF, "h")],
            (at, *out_blocks, gathered),
            "s" + "v" * (len(out_blocks) + 1),
            mix_scratch,
        )
        mixed = exchange(mixed.reshape(groups, sequences, 2 * piece_width), lines)
        mixed = [mixed[number] for number in range(groups)]
    homes = 2 if paired else 1
    members = None
    if paired:
        half = devices // 2
        members = [list(range(half)), list(range(half, devices))]
    side = gated_rows[1:] if paired else []
    after_mix, expert_input, outgoing = local_call(
        functools.partial(send_kernel, pieces=len(mixed)),
        [
            ((sequences, model_width), HALF, "v"),
            ((sequences, model_width), HALF, "v"),
            ((experts_total // homes, homes, tall, slot_width), HALF, "h"),
        ],
        (at, *mixed, held_tokens, hot, *side, gains[0], gains[1]),
        "s" + "v" * (len(mixed) + len(side) + 4),
    )
    outgoing = outgoing.reshape(experts_total // homes, homes * tall, slot_width)
    arrived = exchange(outgoing, members)
    arrived = arrived.reshape(devices // homes, local_count, homes * tall, slot_width)
    answers = []
    for expert in range(local_count):
        (held_gate,) = local_call(
            hold_gate_kernel,
            [(expert_gate.shape[1:], HALF, "v")],
            (after_mix, expert_gate[expert]),
            "vh",
            scratch=[pltpu.SemaphoreType.DMA],
        )
        (answer,) = local_call(
            expert_kernel,
            [((fold, devices // fold, tall, slot_width), HALF, "h")],
            (
                arrived[:, expert].reshape(devices // fold, fold, tall, slot_width),
                held_gate,
                expert_up[expert],
                expert_down[expert],
            ),
            "vvhh",
            scratch=[
                pltpu.VMEM(expert_up.shape[1:], HALF),
                pltpu.VMEM(expert_down.shape[1:], HALF),
                pltpu.SemaphoreType.DMA((2 * fold,)),
            ],
        )
        if not paired:
            answer = answer.swapaxes(0, 1)
        answers.append(answer.reshape(devices, tall, slot_width))
    answered = jnp.stack(answers, axis=1).reshape(experts_total, tall, slot_width)
    returned = exchange(answered)

    (shared_out,) = local_call(
        shared_kernel,
        [((sequences, model_width), WIDE, "v")],
        (expert_input, shared_gate, shared_up, shared_down),
    )
    key_rows, value_rows = keys.swapaxes(0, 1), values.swapaxes(0, 1)
    next_memory = (
        keep_old[..., None, None] * memory_state
        + write_new[..., None, None] * value_rows[..., :, None] * key_rows[..., None, :]
    )
    next_normalizer = keep_old[..., None] * normalizer + write_new[..., None] * key_rows
    (next_tokens,) = local_call(
        final_kernel,
        [((sequences, model_width), HALF, "h")],
        (returned.reshape(slot_count, slot_width), pick, shared_out, after_mix, gains[2]),
    )
    return (next_tokens, next_memory, next_normalizer, next_stabilizer)


def solution(mesh):
    in_specs = (
        P("ep", None),
        P(),
        P(),
        P(),
        P(),
        P("ep", None),
        P("ep", None),
        P("ep", None),
        P("ep", None),
        P(),
        P(),
        P(),
        P(),
        P("ep", None, None, None),
        P("ep", None, None),
        P("ep", None),
        P(None, "ep"),
        P("ep", None),
        P("ep", None),
        P("ep", None, None),
        P("ep", None, None),
        P("ep", None, None),
        P(),
        P(),
        P(),
    )
    out_specs = (P("ep", None), P("ep", None, None, None), P("ep", None, None), P("ep", None))

    return jax.shard_map(
        on_device, mesh=mesh, in_specs=in_specs, out_specs=out_specs, check_vma=False
    )
```
